512 devices in a mesh: grp: 2 (over y), fs: 32 (over z, core), tp: 8 (over x).
Axes of the slice: x: 8, y: 2, z: 16, core: 2. Of those that a mesh axis runs over, the one named last changes fastest.
The devices are a block of a 8x8x16 slice.
Arguments:
- tokens: bfloat16 [32768, 2048], P(('grp', 'fs', 'tp')), parts along dimension 0, may hold values from -6 to 6
- up_master: float32 [2048, 4096], P('fs', 'tp'), may hold values from -0.125 to 0.125
- down_master: float32 [4096, 2048], P('fs', 'tp'), may hold values from -0.09375 to 0.09375
- norm_gain: float32 [2048], P('fs'), may hold values from 0.1 to 1.9
Outputs:
- up_weights: bfloat16 [4096, 4096], P('grp', 'tp'), parts along dimension 0
- down_weights: bfloat16 [8192, 2048], P(('grp', 'tp')), parts along dimension 0
- mlp_output: bfloat16 [32768, 2048], P(('grp', 'fs', 'tp')), parts along dimension 0
The draws below stay inside these ranges and needn't reach their ends.
There are 2 independent parts, one for each index of `grp`. The reference program is written for one: setup_inputs(seed, part) draws one part's arguments, and reference() takes and returns one part's arrays. A program takes and returns all parts, laid end to end along the dimension named above; an argument that names none is the same for every part. Nothing has to cross between parts.
All inputs are finite; a program needn't handle non-finite values.
Results may differ from the reference program's by a relative error of at most 0.014.
Values may be sent and summed in bfloat16 or wider, within the bound.
A program may use at most 64 MiB of HBM per device.

```python
import jax
import jax.numpy as jnp
from jax import lax

D = 2048
FF = 4096
TOKENS = 16384
N_TP = 8


def steps_of(stream_key, dims, split, smallest, top_value):
    level = 1.0
    for dim, blocks in split:
        steps = jax.random.uniform(jax.random.fold_in(jax.random.fold_in(stream_key, 6), dim), (blocks,), jnp.float32, smallest / len(split), top_value / len(split))
        level = level * jnp.repeat(jnp.exp(steps), dims[dim] // blocks).reshape((-1,) + (1,) * (len(dims) - 1 - dim))
    return level


def centred(stream_key, shape, deviation, bound, cuts=(), dtype=jnp.bfloat16):
    entries = deviation * jax.random.normal(stream_key, shape, jnp.float32)
    if cuts:
        entries = entries * steps_of(stream_key, shape, cuts, -0.22, 0.18)
    return jnp.clip(entries, -bound, bound).astype(dtype)


def setup_inputs(seed: int = 0, part: int = 0) -> dict:
    keys = jax.random.split(jax.random.key(seed), 5)
    part_splits = jax.random.split(jax.random.fold_in(keys[4], part), 5)
    tokens = centred(part_splits[0], (TOKENS, D), 1.0, 6.0, ((0, 256),))
    up_master = centred(keys[1], (D, FF), D ** -0.5, 0.125, ((0, 32), (1, 8)), jnp.float32)
    down_master = centred(keys[2], (FF, D), FF ** -0.5, 0.09375, ((0, 32), (1, 8)), jnp.float32)
    norm_gain = jnp.clip(1.0 + 0.18 * jax.random.normal(keys[3], (D,), jnp.float32), 0.1, 1.9)
    return dict(tokens=tokens, up_master=up_master, down_master=down_master, norm_gain=norm_gain)


def reference(tokens, up_master, down_master, norm_gain):
    up_weights = (norm_gain[:, None] * up_master).astype(jnp.bfloat16)
    down_weights = down_master.astype(jnp.bfloat16)
    float_tokens = tokens.astype(jnp.float32)
    scale = lax.rsqrt(lax.optimization_barrier(jnp.mean(float_tokens * float_tokens, axis=-1, keepdims=True)) + 1e-06)
    normed = (float_tokens * scale).astype(jnp.bfloat16)
    preact = jnp.dot(normed, up_weights, preferred_element_type=jnp.float32)
    rectified = jax.nn.relu(preact)
    hidden = (rectified * rectified).astype(jnp.bfloat16)
    row_total = hidden.shape[0]
    block_width = FF // N_TP
    hidden_blocks = hidden.reshape(row_total, N_TP, block_width).transpose(1, 0, 2)
    down_blocks = down_weights.reshape(N_TP, block_width, D)

    def accumulate(running, operands):
        hidden_block, down_block = operands
        partial_value = jnp.dot(hidden_block, down_block, preferred_element_type=jnp.float32).astype(jnp.bfloat16)
        partial_value = lax.optimization_barrier(partial_value)
        return (running + partial_value.astype(jnp.float32), None)
    start_sum = jnp.zeros((row_total, D), jnp.float32)
    summed, _ = lax.scan(accumulate, start_sum, (hidden_blocks, down_blocks))
    return (up_weights, down_weights, summed.astype(jnp.bfloat16))
```

```python
import functools

import jax
import jax.numpy as jnp
from jax import lax
from jax.experimental import pallas as pl
from jax.experimental.pallas import tpu as pltpu
from jax.sharding import PartitionSpec as P

MESH = pl.DeviceIdType.MESH
BF16 = jnp.bfloat16
F32 = jnp.float32
QUARTERS = 4
DOWN_LAG = 3


def message_numbers(n_z, n_x):
    names = ["perm"]
    half_x = n_x // 2
    names += [("tok", way, m) for way in (1, -1) for m in range(2 * half_x - 1)]
    half_z = n_z // 2
    names += [("up", 1, m) for m in range(half_z)] + [("up", -1, m) for m in range(half_z - 1)]
    names += [("dn", 1, m) for m in range(half_z - 1)] + [("dn", -1, m) for m in range(half_z)]
    names += [(kind + "pair", way, m) for kind in ("up", "dn") for way in (1, -1) for m in range(half_z + 1)]
    names += [
        ("rs", way, q, k)
        for way in (1, -1)
        for q in range(QUARTERS)
        for k in range(chain_start(q, way, half_x), 0, -1)
    ]
    return {name: number for number, name in enumerate(names)}


def chain_start(q, way, half_x):
    return half_x if (q % 2 == 0) == (way == 1) else half_x - 1


def kernel(
    number, slot, n_f, n_x,
    tok_in, up_in, dn_in, gain_in,
    up_out, dn_out, y_out,
    tok_v, up_v, dn_v, gain_v, stage, tok_all, up_all, dn_all, hid, part, rs_out, rs_in, y_v,
    send_sem, recv_sem, load_sem, store_sem,
):
    x = lax.axis_index("tp")
    f = lax.axis_index("fs")
    z, core = f // 2, f % 2
    n_z, half_x = n_f // 2, n_x // 2
    half_z = n_z // 2
    rows, d = tok_in.shape
    up_rows, width = up_in.shape
    dn_rows, dn_cols = dn_in.shape
    half = rows // 2
    q_cols = d // QUARTERS

    def at(**where):
        return {"fs": f, "tp": x} | where

    x_peer = {way: at(tp=lax.rem(x + way + n_x, n_x)) for way in (1, -1)}
    z_peer = {way: at(fs=lax.rem(f + 2 * way + n_f, n_f)) for way in (1, -1)}
    pair = at(fs=2 * z + 1 - core)
    z_hi, z_lo = z // 2, z % 2
    perm_f = (2 * x + z_lo) * 2 + core
    perm_peer = at(tp=z_hi, fs=perm_f)
    stays = z_hi == x

    barrier = pltpu.get_barrier_semaphore()
    for peer in (x_peer[1], x_peer[-1], z_peer[1], z_peer[-1], pair):
        pl.semaphore_signal(barrier, inc=1, device_id=peer, device_id_type=MESH)

    @pl.when(jnp.logical_not(stays))
    def _():
        pl.semaphore_signal(barrier, inc=1, device_id=perm_peer, device_id_type=MESH)

    loads = [
        pltpu.make_async_copy(src, dst, load_sem.at[k])
        for k, (src, dst) in enumerate(((dn_in, dn_v), (tok_in, tok_v), (gain_in, gain_v), (up_in, up_v)))
    ]
    for load in loads:
        load.start()

    def up_at(zz, cc):
        return up_all.at[pl.ds(pl.multiple_of((zz * 2 + cc) * up_rows, up_rows), up_rows), :]

    def dn_at(zz, cc):
        row = pl.multiple_of((lax.rem(zz, 2) * 2 + cc) * dn_rows, dn_rows)
        col = pl.multiple_of((zz // 2) * dn_cols, dn_cols)
        return dn_all.at[pl.ds(row, dn_rows), pl.ds(col, dn_cols)]

    def tok_at(xx, part_of):
        return tok_all.at[pl.ds(pl.multiple_of(xx * rows + part_of * half, half), half), :]

    def message(name, src, dst, peer):
        return pltpu.make_async_remote_copy(
            src_ref=src,
            dst_ref=dst,
            send_sem=send_sem.at[number[name]],
            recv_sem=recv_sem.at[number[name]],
            device_id=peer,
            device_id_type=MESH,
        )

    sent = []

    def send(name, src, dst, peer):
        copy = message(name, src, dst, peer)
        copy.start()
        sent.append(copy)

    loads[0].wait()
    stage[...] = dn_v[...].astype(BF16)
    loads[1].wait()
    tokens = tok_v[...].astype(F32)
    scale = lax.rsqrt(jnp.mean(tokens * tokens, axis=-1, keepdims=True) + 1e-06)
    tok_all[pl.ds(pl.multiple_of(x * rows, rows), rows), :] = (tokens * scale).astype(BF16)
    loads[2].wait()
    loads[3].wait()
    diagonal = lax.broadcasted_iota(jnp.int32, (up_rows, up_rows), 0) == lax.broadcasted_iota(
        jnp.int32, (up_rows, up_rows), 1
    )
    gain = jnp.sum(
        jnp.where(diagonal, jnp.broadcast_to(gain_v[...], (up_rows, up_rows)), 0.0), axis=1, keepdims=True
    )
    up_all[pl.ds(pl.multiple_of(f * up_rows, up_rows), up_rows), :] = (gain * up_v[...]).astype(BF16)

    @pl.when(stays)
    def _():
        row = pl.multiple_of((z_lo * 2 + core) * dn_rows, dn_rows)
        col = pl.multiple_of(x * dn_cols, dn_cols)
        dn_all[pl.ds(row, dn_rows), pl.ds(col, dn_cols)] = stage[...]

    pl.semaphore_wait(barrier, jnp.where(stays, 5, 6))

    @pl.when(jnp.logical_not(stays))
    def _():
        row = pl.multiple_of((z_lo * 2 + core) * dn_rows, dn_rows)
        col = pl.multiple_of(x * dn_cols, dn_cols)
        message("perm", stage, dn_all.at[pl.ds(row, dn_rows), pl.ds(col, dn_cols)], perm_peer).start()

    def z_of(way, m):
        return lax.rem(z - way * m + n_z, n_z)

    def x_of(way, m):
        return lax.rem(x - way * m + n_x, n_x)

    def tok_block(way, m, receiver):
        part_of = m % 2 if way == 1 else 1 - m % 2
        return tok_at(x_of(way, m // 2 + receiver), part_of)

    def send_tok(way, m):
        block = tok_block(way, m, 0)
        send(("tok", way, m), block, block, x_peer[way])

    def weights(kind, place, limits):
        def forward(way, m):
            if m < limits[way]:
                block = place(z_of(way, m), core)
                send((kind, way, m), block, block, z_peer[way])

        def to_pair(way, m):
            block = place(z_of(way, m), core)
            send((kind + "pair", way, m), block, block, pair)

        def first():
            forward(1, 0)
            forward(-1, 0)
            to_pair(1, 0)

        def arrived(way, m):
            if m < limits[way]:
                block = place(z_of(way, m + 1), core)
                message((kind, way, m), block, block, z_peer[way]).wait_recv()
                forward(way, m + 1)
                to_pair(way, m + 1)

        def from_pair():
            for way in (1, -1):
                for m in range(1 if way == -1 else 0, limits[way] + 1):
                    block = place(z_of(way, m), 1 - core)
                    message((kind + "pair", way, m), block, block, pair).wait_recv()

        return first, arrived, from_pair

    up_first, up_arrived, up_from_pair = weights("up", up_at, {1: half_z, -1: half_z - 1})
    dn_first, dn_arrived, dn_from_pair = weights("dn", dn_at, {1: half_z - 1, -1: half_z})
    last_tok = 2 * half_x - 1

    for way in (1, -1):
        send_tok(way, 0)
    up_first()
    for way in (1, -1):
        send_tok(way, 1)

    pieces = 4
    piece = (n_x * rows) // pieces

    def hidden_piece(p):
        block = pl.ds(p * piece, piece)
        product = jnp.dot(tok_all[block, :], up_all[...], preferred_element_type=F32)
        rectified = jnp.maximum(product, 0.0)
        hid[block, :] = (rectified * rectified).astype(BF16)

    up_store = pltpu.make_async_copy(up_all, up_out, store_sem.at[0])
    dn_store = pltpu.make_async_copy(dn_all, dn_out, store_sem.at[1])
    done = 0
    for tick in range(1, half_z + DOWN_LAG + 1):
        m = tick - 1
        for way in (1, -1):
            up_arrived(way, m)
        if m < last_tok:
            for way in (1, -1):
                block = tok_block(way, m, 1)
                message(("tok", way, m), block, block, x_peer[way]).wait_recv()
                if m + 2 < last_tok:
                    send_tok(way, m + 2)
        if tick == DOWN_LAG:

            @pl.when(jnp.logical_not(stays))
            def _():
                block = dn_at(z, core)
                message("perm", stage, block, perm_peer).wait()

            dn_first()
        if tick > DOWN_LAG:
            for way in (1, -1):
                dn_arrived(way, tick - DOWN_LAG - 1)
        if tick == half_z:
            up_from_pair()
            up_store.start()
        if tick >= half_z and done < pieces:
            hidden_piece(done)
            done += 1
    while done < pieces:
        hidden_piece(done)
        done += 1
    dn_from_pair()
    dn_store.start()

    def rs_rows(xx):
        return pl.ds(pl.multiple_of(xx * rows, rows), rows)

    def send_rs(way, q, k):
        where = slot[(way, q, k)]
        total = part[q, rs_rows(lax.rem(x + way * k + n_x, n_x)), :]
        if k < chain_start(q, way, half_x):
            before = slot[(way, q, k + 1)]
            message(("rs", way, q, k + 1), rs_out.at[before], rs_in.at[before], x_peer[way]).wait_recv()
            total = total + rs_in[before].astype(F32)
        rs_out[where] = total.astype(BF16)
        send(("rs", way, q, k), rs_out.at[where], rs_in.at[where], x_peer[way])

    for q in range(QUARTERS):
        part[q] = jnp.dot(hid[...], dn_all[:, q * q_cols : (q + 1) * q_cols], preferred_element_type=F32)
        for way in (1, -1):
            send_rs(way, q, chain_start(q, way, half_x))
    for later in range(1, half_x):
        for q in range(QUARTERS):
            for way in (1, -1):
                k = chain_start(q, way, half_x) - later
                if k >= 1:
                    send_rs(way, q, k)
    for q in range(QUARTERS):
        total = part[q, rs_rows(x), :]
        for way in (1, -1):
            last = slot[(way, q, 1)]
            message(("rs", way, q, 1), rs_out.at[last], rs_in.at[last], x_peer[way]).wait_recv()
            total = total + rs_in[last].astype(F32)
        y_v[:, q * q_cols : (q + 1) * q_cols] = total.astype(BF16)
    y_store = pltpu.make_async_copy(y_v, y_out, store_sem.at[2])
    y_store.start()
    for copy in sent:
        copy.wait_send()
    up_store.wait()
    dn_store.wait()
    y_store.wait()


def solution(mesh):
    n_f, n_x = mesh.shape["fs"], mesh.shape["tp"]
    assert n_f == 4 * n_x
    number = message_numbers(n_f // 2, n_x)
    slots = [name[1:] for name in number if name[0] == "rs"]
    slot = {name: k for k, name in enumerate(slots)}

    def on_device(tokens, up_master, down_master, norm_gain):
        rows, d = tokens.shape
        up_rows, width = up_master.shape
        dn_rows, dn_cols = down_master.shape
        any_space = pl.BlockSpec(memory_space=pl.ANY)
        return pl.pallas_call(
            functools.partial(kernel, number, slot, n_f, n_x),
            out_shape=(
                jax.ShapeDtypeStruct((up_rows * n_f, width), BF16),
                jax.ShapeDtypeStruct((width, d), BF16),
                jax.ShapeDtypeStruct((rows, d), BF16),
            ),
            in_specs=[any_space] * 4,
            out_specs=(any_space,) * 3,
            scratch_shapes=[
                pltpu.VMEM((rows, d), BF16),
                pltpu.VMEM((up_rows, width), F32),
                pltpu.VMEM((dn_rows, dn_cols), F32),
                pltpu.VMEM((1, up_rows), F32),
                pltpu.VMEM((dn_rows, dn_cols), BF16),
                pltpu.VMEM((n_x * rows, d), BF16),
                pltpu.VMEM((up_rows * n_f, width), BF16),
                pltpu.VMEM((width, d), BF16),
                pltpu.VMEM((n_x * rows, width), BF16),
                pltpu.VMEM((QUARTERS, n_x * rows, d // QUARTERS), F32),
                pltpu.VMEM((len(slots), rows, d // QUARTERS), BF16),
                pltpu.VMEM((len(slots), rows, d // QUARTERS), BF16),
                pltpu.VMEM((rows, d), BF16),
                pltpu.SemaphoreType.DMA((len(number),)),
                pltpu.SemaphoreType.DMA((len(number),)),
                pltpu.SemaphoreType.DMA((4,)),
                pltpu.SemaphoreType.DMA((3,)),
            ],
            compiler_params=pltpu.CompilerParams(
                collective_id=0, has_side_effects=True, vmem_limit_bytes=48 * 1024 * 1024
            ),
            name="handoff",
        )(tokens, up_master, down_master, norm_gain.reshape(1, up_rows))

    in_specs = (P(("grp", "fs", "tp"), None), P("fs", "tp"), P("fs", "tp"), P("fs"))
    out_specs = (P("grp", "tp"), P(("grp", "tp"), None), P(("grp", "fs", "tp"), None))
    return jax.shard_map(on_device, mesh=mesh, in_specs=in_specs, out_specs=out_specs, check_vma=False)
```

```python
import functools

import jax
import jax.numpy as jnp
from jax import lax
from jax.experimental import pallas as pl
from jax.experimental.pallas import tpu as pltpu
from jax.sharding import PartitionSpec as P

MESH = pl.DeviceIdType.MESH
BF16 = jnp.bfloat16
F32 = jnp.float32
QUARTERS = 4
DOWN_LAG = 4
TOK_CHUNKS = 4
WEIGHT_CHUNKS = 2
WAYS = (1, -1)
COPY_BYTES = 512 * 1024


def ring_messages(n, chunks):
    return (n // 2 - 1) * chunks + chunks // 2


def chunk_of(way, m, chunks):
    return (m + (0 if way == 1 else chunks // 2)) % chunks


def chain_start(j, way, half_x):
    return half_x if (j % 2 == 0) == (way == 1) else half_x - 1


SEND_SEMS = ("perm", "tok", "up", "dn", "uppair", "dnpair", "rs")


def receive_numbers(n_z, n_x):
    names = ["perm"]
    names += [("tok", way, m) for way in WAYS for m in range(ring_messages(n_x, TOK_CHUNKS))]
    for kind in ("up", "dn"):
        names += [(kind, way, m) for way in WAYS for m in range(ring_messages(n_z, WEIGHT_CHUNKS))]
    names += [("uppair", 0)] + [("dnpair", group) for group in range(QUARTERS)]
    names += [
        ("rs", way, j, k)
        for way in WAYS
        for j in range(QUARTERS)
        for k in range(chain_start(j, way, n_x // 2), 0, -1)
    ]
    return {name: number for number, name in enumerate(names)}


def kernel(
    number, slot, n_f, n_x,
    tok_in, up_in, dn_in, gain_in,
    up_out, dn_out, y_out,
    up_all, dn_all, y_v, tok_v, up_v, dn_v, gain_v, stage, tok_all, hid, part, rs_out, rs_in,
    send_sem, recv_sem, load_sem,
):
    x = lax.axis_index("tp")
    f = lax.axis_index("fs")
    z, core = f // 2, f % 2
    n_z, half_x = n_f // 2, n_x // 2
    rows, d = tok_in.shape
    up_rows, width = up_in.shape
    dn_rows, dn_cols = dn_in.shape
    q_cols = d // QUARTERS

    def at(**where):
        return {"fs": f, "tp": x} | where

    x_peer = {way: at(tp=lax.rem(x + way + n_x, n_x)) for way in WAYS}
    z_peer = {way: at(fs=lax.rem(f + 2 * way + n_f, n_f)) for way in WAYS}
    pair = at(fs=2 * z + 1 - core)
    z_hi, z_lo = z // 2, z % 2
    perm_peer = at(tp=z_hi, fs=(2 * x + z_lo) * 2 + core)
    stays = z_hi == x

    barrier = pltpu.get_barrier_semaphore()
    for peer in (x_peer[1], x_peer[-1], z_peer[1], z_peer[-1], pair):
        pl.semaphore_signal(barrier, inc=1, device_id=peer, device_id_type=MESH)

    @pl.when(jnp.logical_not(stays))
    def _():
        pl.semaphore_signal(barrier, inc=1, device_id=perm_peer, device_id_type=MESH)

    loads = [
        pltpu.make_async_copy(src, dst, load_sem.at[k])
        for k, (src, dst) in enumerate(((dn_in, dn_v), (tok_in, tok_v), (gain_in, gain_v), (up_in, up_v)))
    ]
    for load in loads:
        load.start()

    def up_at(zz, cc, c):
        size = up_rows // WEIGHT_CHUNKS
        return up_all.at[pl.ds(pl.multiple_of((zz * 2 + cc) * up_rows + c * size, size), size), :]

    def dn_at(zz, cc, c=None):
        size = dn_rows if c is None else dn_rows // WEIGHT_CHUNKS
        row = pl.multiple_of((lax.rem(zz, 2) * 2 + cc) * dn_rows + (0 if c is None else c * size), size)
        col = pl.multiple_of((zz // 2) * dn_cols, dn_cols)
        return dn_all.at[pl.ds(row, size), pl.ds(col, dn_cols)]

    def tok_at(xx, c):
        size = rows // TOK_CHUNKS
        return tok_all.at[pl.ds(pl.multiple_of(xx * rows + c * size, size), size), :]

    def message(name, src, dst, peer):
        return pltpu.make_async_remote_copy(
            src_ref=src,
            dst_ref=dst,
            send_sem=send_sem.at[SEND_SEMS.index(name if name == "perm" else name[0])],
            recv_sem=recv_sem.at[number[name]],
            device_id=peer,
            device_id_type=MESH,
        )

    def send(name, src, dst, peer):
        message(name, src, dst, peer).start()

    def wait_bytes(sem, ref):
        pltpu.make_async_copy(ref, ref, sem).wait()

    with jax.named_scope("own"):
        loads[0].wait()
        stage[...] = dn_v[...].astype(BF16)

        @pl.when(stays)
        def _():
            dn_all[
                pl.ds(pl.multiple_of((z_lo * 2 + core) * dn_rows, dn_rows), dn_rows),
                pl.ds(pl.multiple_of(x * dn_cols, dn_cols), dn_cols),
            ] = stage[...]

        loads[1].wait()
        tokens = tok_v[...].astype(F32)
        scale = lax.rsqrt(jnp.mean(tokens * tokens, axis=-1, keepdims=True) + 1e-06)
        tok_all[pl.ds(pl.multiple_of(x * rows, rows), rows), :] = (tokens * scale).astype(BF16)
        loads[2].wait()
        loads[3].wait()
        square = (up_rows, up_rows)
        diagonal = lax.broadcasted_iota(jnp.int32, square, 0) == lax.broadcasted_iota(jnp.int32, square, 1)
        gain = jnp.sum(jnp.where(diagonal, jnp.broadcast_to(gain_v[...], square), 0.0), axis=1, keepdims=True)
        up_all[pl.ds(pl.multiple_of(f * up_rows, up_rows), up_rows), :] = (gain * up_v[...]).astype(BF16)

    with jax.named_scope("barrier"):
        pl.semaphore_wait(barrier, jnp.where(stays, 5, 6))

    @pl.when(jnp.logical_not(stays))
    def _():
        dst = dn_all.at[
            pl.ds(pl.multiple_of((z_lo * 2 + core) * dn_rows, dn_rows), dn_rows),
            pl.ds(pl.multiple_of(x * dn_cols, dn_cols), dn_cols),
        ]
        message("perm", stage, dst, perm_peer).start()

    def stream(kind, n, chunks, me, place, peers, groups):
        count = ring_messages(n, chunks)
        to_pair = bool(groups)

        def group_of(m):
            return sum(m >= stop for stop in groups)

        def block(way, m, away, other=False):
            owner = lax.rem(me - way * (m // chunks + away) + n, n)
            return place(owner, 1 - core if other else core, chunk_of(way, m, chunks))

        def forward(way, m):
            if m < count:
                ref = block(way, m, 0)
                send((kind, way, m), ref, ref, peers[way])

        def first():
            for m in range(chunks):
                for way in WAYS:
                    forward(way, m)
            if to_pair:
                for c in range(chunks):
                    ref = place(me, core, c)
                    send((kind + "pair", 0), ref, ref, pair)

        def step(m):
            if 0 <= m < count:
                with jax.named_scope(f"{kind}{m}"):
                    for way in WAYS:
                        ref = block(way, m, 1)
                        message((kind, way, m), ref, ref, peers[way]).wait_recv()
                        forward(way, m + chunks)
                        if to_pair:
                            send((kind + "pair", group_of(m)), ref, ref, pair)

        def from_pair(group, whole):
            start = groups[group - 1] if group else 0
            blocks = 2 * (groups[group] - start) + (chunks if group == 0 else 0)
            size = blocks * place(0, 0, 0).shape[0] * place(0, 0, 0).shape[1]
            with jax.named_scope(f"{kind}pair{group}"):
                wait_bytes(
                    recv_sem.at[number[(kind + "pair", group)]], whole.at[pl.ds(0, size // whole.shape[1]), :]
                )

        return count, first, step, from_pair

    tok_count, tok_first, tok_step, _ = stream(
        "tok", n_x, TOK_CHUNKS, x, lambda xx, cc, c: tok_at(xx, c), x_peer, ()
    )
    last = ring_messages(n_z, WEIGHT_CHUNKS)
    ready_at = [distance * WEIGHT_CHUNKS for distance in (3, 5, 7)] + [last]
    up_count, up_first, up_step, up_from_pair = stream("up", n_z, WEIGHT_CHUNKS, z, up_at, z_peer, (last,))
    dn_count, dn_first, dn_step, dn_from_pair = stream("dn", n_z, WEIGHT_CHUNKS, z, dn_at, z_peer, ready_at)

    tok_first()
    up_first()

    pieces = 4
    piece = (n_x * rows) // pieces

    def hidden_piece(p):
        with jax.named_scope(f"hid{p}"):
            block = pl.ds(p * piece, piece)
            product = jnp.dot(tok_all[block, :], up_all[...], preferred_element_type=F32)
            rectified = jnp.maximum(product, 0.0)
            hid[block, :] = (rectified * rectified).astype(BF16)

    for tick in range(max(tok_count, up_count)):
        up_step(tick)
        tok_step(tick)
        if tick == DOWN_LAG - 1:
            with jax.named_scope("perm"):

                @pl.when(jnp.logical_not(stays))
                def _():
                    message("perm", stage, dn_at(z, core), perm_peer).wait()

                dn_first()
        dn_step(tick - DOWN_LAG)
    down = max(tok_count, up_count) - DOWN_LAG
    up_from_pair(0, up_all)
    up_store = pltpu.make_async_copy(up_all, up_out, load_sem.at[0])
    up_store.start()
    for p in range(pieces):
        hidden_piece(p)
        if p < pieces - 1 and down < 10:
            dn_step(down)
            down += 1

    near = 2 * (lax.rem(z, QUARTERS) // 2) - 1
    own_quarter = z // QUARTERS
    quarter = [
        lax.rem(own_quarter + QUARTERS + shift, QUARTERS) for shift in (0, near, -near, 2)
    ]
    def columns(j):
        return pl.ds(pl.multiple_of(quarter[j] * q_cols, q_cols), q_cols)

    def rs_rows(xx):
        return pl.ds(pl.multiple_of(xx * rows, rows), rows)

    def send_rs(way, j, k):
        where = slot[(way, j, k)]
        total = part[j, rs_rows(lax.rem(x + way * k + n_x, n_x)), :]
        if k < chain_start(j, way, half_x):
            before = slot[(way, j, k + 1)]
            message(("rs", way, j, k + 1), rs_out.at[before], rs_in.at[before], x_peer[way]).wait_recv()
            total = total + rs_in[before].astype(F32)
        rs_out[where] = total.astype(BF16)
        send(("rs", way, j, k), rs_out.at[where], rs_in.at[where], x_peer[way])

    def begin(j):
        dn_from_pair(j, dn_all)
        with jax.named_scope(f"part{j}"):
            part[j] = jnp.dot(hid[...], dn_all[:, columns(j)], preferred_element_type=F32)
        for way in WAYS:
            send_rs(way, j, chain_start(j, way, half_x))

    def go_on(j, later):
        with jax.named_scope(f"rs{j}r{later}"):
            for way in WAYS:
                k = chain_start(j, way, half_x) - later
                if k >= 1:
                    send_rs(way, j, k)

    def end(j):
        with jax.named_scope(f"end{j}"):
            total = part[j, rs_rows(x), :]
            for way in WAYS:
                last = slot[(way, j, 1)]
                message(("rs", way, j, 1), rs_out.at[last], rs_in.at[last], x_peer[way]).wait_recv()
                total = total + rs_in[last].astype(F32)
            y_v[:, columns(j)] = total.astype(BF16)

    def more_down(stop):
        nonlocal down
        while down < stop:
            dn_step(down)
            down += 1

    more_down(ready_at[0])
    begin(0)
    more_down(ready_at[1])
    begin(1)
    more_down(11)
    go_on(0, 1)
    more_down(12)
    go_on(1, 1)
    more_down(13)
    go_on(0, 2)
    more_down(ready_at[2])
    begin(2)
    go_on(1, 2)
    more_down(ready_at[3])
    begin(3)
    dn_store = pltpu.make_async_copy(dn_all, dn_out, load_sem.at[1])
    dn_store.start()
    for j, later in ((0, 3), (1, 3), (2, 1), (3, 1)):
        go_on(j, later)
    end(0)
    end(1)
    for j, later in ((2, 2), (3, 2), (2, 3), (3, 3)):
        go_on(j, later)
    end(2)
    end(3)
    y_store = pltpu.make_async_copy(y_v, y_out, load_sem.at[2])
    y_store.start()
    with jax.named_scope("drain"):
        ring_rows = 2 * up_count * (up_rows // WEIGHT_CHUNKS)
        for kind, ref in (
            ("tok", tok_all.at[pl.ds(0, 2 * tok_count * (rows // TOK_CHUNKS)), :]),
            ("up", up_all.at[pl.ds(0, ring_rows), :]),
            ("uppair", up_all.at[pl.ds(0, n_z * up_rows), :]),
            ("dn", dn_all.at[pl.ds(0, ring_rows * width // d), :]),
            ("dnpair", dn_all.at[pl.ds(0, n_z * up_rows * width // d), :]),
            ("rs", rs_out),
        ):
            wait_bytes(send_sem.at[SEND_SEMS.index(kind)], ref)
        up_store.wait()
        dn_store.wait()
        y_store.wait()


def copier(up_in, dn_in, y_in, up_out, dn_out, y_out, up_v, dn_v, y_v, sem_in, sem_out):
    moves = []
    for src, mid, dst in ((up_in, up_v, up_out), (dn_in, dn_v, dn_out), (y_in, y_v, y_out)):
        size = min(src.shape[0], COPY_BYTES // (2 * src.shape[1]))
        for start in range(0, src.shape[0], size):
            part = pl.ds(start, size)
            k = len(moves)
            moves.append(
                (
                    pltpu.make_async_copy(src.at[part, :], mid.at[part, :], sem_in.at[k]),
                    pltpu.make_async_copy(mid.at[part, :], dst.at[part, :], sem_out.at[k]),
                )
            )
    for load, _ in moves:
        load.start()
    for load, store in moves:
        load.wait()
        store.start()
    for _, store in moves:
        store.wait()


def solution(mesh):
    n_f, n_x = mesh.shape["fs"], mesh.shape["tp"]
    assert n_f == 4 * n_x and n_x == 8
    number = receive_numbers(n_f // 2, n_x)
    slots = [name[1:] for name in number if name[0] == "rs"]
    slot = {name: k for k, name in enumerate(slots)}

    def on_device(tokens, up_master, down_master, norm_gain):
        rows, d = tokens.shape
        up_rows, width = up_master.shape
        dn_rows, dn_cols = down_master.shape
        results = (
            jax.ShapeDtypeStruct((up_rows * n_f, width), BF16),
            jax.ShapeDtypeStruct((width, d), BF16),
            jax.ShapeDtypeStruct((rows, d), BF16),
        )
        in_hbm = pl.BlockSpec(memory_space=pltpu.HBM)
        made = pl.pallas_call(
            functools.partial(kernel, number, slot, n_f, n_x),
            out_shape=results,
            in_specs=[in_hbm] * 4,
            out_specs=(in_hbm,) * 3,
            scratch_shapes=[
                *(pltpu.VMEM(result.shape, BF16) for result in results),
                pltpu.VMEM((rows, d), BF16),
                pltpu.VMEM((up_rows, width), F32),
                pltpu.VMEM((dn_rows, dn_cols), F32),
                pltpu.VMEM((1, up_rows), F32),
                pltpu.VMEM((dn_rows, dn_cols), BF16),
                pltpu.VMEM((n_x * rows, d), BF16),
                pltpu.VMEM((n_x * rows, width), BF16),
                pltpu.VMEM((QUARTERS, n_x * rows, d // QUARTERS), F32),
                pltpu.VMEM((len(slots), rows, d // QUARTERS), BF16),
                pltpu.VMEM((len(slots), rows, d // QUARTERS), BF16),
                pltpu.SemaphoreType.DMA((len(SEND_SEMS),)),
                pltpu.SemaphoreType.DMA((len(number),)),
                pltpu.SemaphoreType.DMA((4,)),
            ],
            compiler_params=pltpu.CompilerParams(
                collective_id=0, has_side_effects=True, vmem_limit_bytes=62 * 1024 * 1024
            ),
            name="handoff",
        )(tokens, up_master, down_master, norm_gain.reshape(1, up_rows))
        copies = sum(pl.cdiv(2 * result.size, COPY_BYTES) for result in results)
        return pl.pallas_call(
            copier,
            out_shape=results,
            in_specs=[in_hbm] * 3,
            out_specs=(in_hbm,) * 3,
            scratch_shapes=[
                *(pltpu.VMEM(result.shape, BF16) for result in results),
                pltpu.SemaphoreType.DMA((copies,)),
                pltpu.SemaphoreType.DMA((copies,)),
            ],
            compiler_params=pltpu.CompilerParams(vmem_limit_bytes=62 * 1024 * 1024),
            name="hand_out",
        )(*made)

    in_specs = (P(("grp", "fs", "tp"), None), P("fs", "tp"), P("fs", "tp"), P("fs"))
    out_specs = (P("grp", "tp"), P(("grp", "tp"), None), P(("grp", "fs", "tp"), None))
    return jax.shard_map(on_device, mesh=mesh, in_specs=in_specs, out_specs=out_specs, check_vma=False)
```

```python
import functools

import jax
import jax.numpy as jnp
from jax import lax
from jax.experimental import pallas as pl
from jax.experimental.pallas import tpu as pltpu
from jax.sharding import PartitionSpec as P

MESH = pl.DeviceIdType.MESH
BF16 = jnp.bfloat16
F32 = jnp.float32
QUARTERS = 4
DOWN_LAG = 9
TOK_CHUNKS = 4
WEIGHT_CHUNKS = 2
WAYS = (1, -1)
SEND_SEMS = ("own", "perm", "across", "tok", "tokpair", "up", "uppair", "dn", "dnpair", "rs")


def ring_messages(n, chunks):
    return (n // 2 - 1) * chunks + chunks // 2


def chunk_of(way, m, chunks):
    return (m + (0 if way == 1 else chunks // 2)) % chunks


def chain_start(j, way, half_x):
    return half_x if (j % 2 == 0) == (way == 1) else half_x - 1


def receive_numbers(n_z, n_x):
    names = [("own",), ("perm",), ("across",), ("tokpair", 0), ("uppair", 0)]
    names += [("dnpair", group) for group in range(QUARTERS)]
    names += [("tok", way, m) for way in WAYS for m in range(ring_messages(n_x, TOK_CHUNKS))]
    for kind in ("up", "dn"):
        names += [(kind, way, m) for way in WAYS for m in range(ring_messages(n_z, WEIGHT_CHUNKS))]
    names += [
        ("rs", way, j, k)
        for way in WAYS
        for j in range(QUARTERS)
        for k in range(chain_start(j, way, n_x // 2), 0, -1)
    ]
    return {name: number for number, name in enumerate(names)}


def kernel(
    number, slot, n_f, n_x,
    tok_in, up_in, dn_in, gain_in,
    up_all, dn_all, y_out,
    tok_v, up_v, dn_v, gain_v, stage, tok_all, hid, part, rs_out, rs_in,
    send_sem, recv_sem, load_sem,
):
    x = lax.axis_index("tp")
    f = lax.axis_index("fs")
    z, core = f // 2, f % 2
    n_z, half_x = n_f // 2, n_x // 2
    rows, d = tok_in.shape
    up_rows, width = up_in.shape
    dn_rows, dn_cols = dn_in.shape
    q_cols = d // QUARTERS
    all_rows = n_x * rows

    group = lax.axis_index("grp")
    odd = group % 2

    def at(**where):
        return {"grp": group, "fs": f, "tp": x} | where

    x_peer = {way: at(tp=lax.rem(x + way + n_x, n_x)) for way in WAYS}
    z_peer = {way: at(fs=lax.rem(f + 2 * way + n_f, n_f)) for way in WAYS}
    pair = at(fs=2 * z + 1 - core)
    z_hi, z_lo = z // 2, z % 2
    perm_chip = 2 * x + z_lo
    perm_peer = at(tp=z_hi, fs=perm_chip * 2 + 1)
    stays = z_hi == x
    moves = jnp.logical_not(stays)
    permutes = core == odd
    across = at(grp=group + 1 - 2 * odd)

    def greet(peer):
        pl.semaphore_signal(barrier, inc=1, device_id=peer, device_id_type=MESH)

    barrier = pltpu.get_barrier_semaphore()
    for peer in (x_peer[1], x_peer[-1], pair):
        greet(peer)

    @pl.when(core == 1)
    def _():
        for way in WAYS:
            greet(z_peer[way])
        greet(across)

        @pl.when(moves)
        def _():
            greet(at(tp=z_hi, fs=perm_chip * 2 + odd))

    loads = [
        pltpu.make_async_copy(src, dst, load_sem.at[k])
        for k, (src, dst) in enumerate(((dn_in, dn_v), (tok_in, tok_v), (gain_in, gain_v), (up_in, up_v)))
    ]
    for load in loads:
        load.start()

    def up_at(zz, c):
        return up_all.at[pl.ds(pl.multiple_of((zz * 2 + c) * up_rows, up_rows), up_rows), :]

    def dn_at(zz, c):
        row = pl.multiple_of((lax.rem(zz, 2) * 2 + c) * dn_rows, dn_rows)
        col = pl.multiple_of((zz // 2) * dn_cols, dn_cols)
        return dn_all.at[pl.ds(row, dn_rows), pl.ds(col, dn_cols)]

    def tok_at(xx, c):
        size = rows // 2
        row = pl.multiple_of((c % 2) * all_rows + xx * rows + (c // 2) * size, size)
        return tok_all.at[pl.ds(row, size), :]

    def tok_own(c):
        return tok_all.at[pl.ds(pl.multiple_of(c * all_rows + x * rows, rows), rows), :]

    def message(name, src, dst, peer):
        return pltpu.make_async_remote_copy(
            src_ref=src,
            dst_ref=dst,
            send_sem=send_sem.at[SEND_SEMS.index(name[0])],
            recv_sem=recv_sem.at[number[name]],
            device_id=peer,
            device_id_type=MESH,
        )

    def send(name, src, dst, peer):
        message(name, src, dst, peer).start()

    def wait_bytes(sem, ref):
        pltpu.make_async_copy(ref, ref, sem).wait()

    with jax.named_scope("own"):
        loads[1].wait()
        tokens = tok_v[...].astype(F32)
        scale = lax.rsqrt(jnp.mean(tokens * tokens, axis=-1, keepdims=True) + 1e-06)
        tok_own(core)[...] = (tokens * scale).astype(BF16)
        loads[0].wait()
        stage[...] = dn_v[...].astype(BF16)
        perm_dst = dn_all.at[
            pl.ds(pl.multiple_of((z_lo * 2 + core) * dn_rows, dn_rows), dn_rows),
            pl.ds(pl.multiple_of(x * dn_cols, dn_cols), dn_cols),
        ]

        @pl.when(jnp.logical_and(stays, jnp.logical_and(permutes, core == 1)))
        def _():
            perm_dst[...] = stage[...]

        loads[2].wait()
        loads[3].wait()
        square = (up_rows, up_rows)
        diagonal = lax.broadcasted_iota(jnp.int32, square, 0) == lax.broadcasted_iota(jnp.int32, square, 1)
        gain = jnp.sum(jnp.where(diagonal, jnp.broadcast_to(gain_v[...], square), 0.0), axis=1, keepdims=True)
        up_at(z, core)[...] = (gain * up_v[...]).astype(BF16)

    with jax.named_scope("barrier"):
        pl.semaphore_wait(barrier, 3 + 3 * core + jnp.where(jnp.logical_and(moves, permutes), 1, 0))

    def stream(kind, n, chunks, me, place, peers, to_pair):
        count = ring_messages(n, chunks)

        def block(way, m, away):
            owner = lax.rem(me - way * (m // chunks + away) + n, n)
            return place(owner, chunk_of(way, m, chunks))

        def forward(way, m):
            if m < count:
                ref = block(way, m, 0)
                send((kind, way, m), ref, ref, peers[way])

        def step(m):
            if 0 <= m < count:
                with jax.named_scope(f"{kind}{m}"):
                    for way in WAYS:
                        ref = block(way, m, 1)
                        message((kind, way, m), ref, ref, peers[way]).wait_recv()
                        forward(way, m + chunks)
                        group = to_pair(way, m)
                        if group is not None:
                            send((kind + "pair", group), ref, ref, pair)

        return count, forward, step

    last = ring_messages(n_z, WEIGHT_CHUNKS)
    ready_at = [distance * WEIGHT_CHUNKS for distance in (3, 5, 7)] + [last]
    tok_count, tok_forward, tok_step = stream(
        "tok", n_x, TOK_CHUNKS, x, tok_at, x_peer,
        lambda way, m: 0 if chunk_of(way, m, TOK_CHUNKS) % 2 else None,
    )
    up_count, up_forward, up_step = stream("up", n_z, WEIGHT_CHUNKS, z, up_at, z_peer, lambda way, m: 0)
    dn_count, dn_forward, dn_step = stream(
        "dn", n_z, WEIGHT_CHUNKS, z, dn_at, z_peer, lambda way, m: sum(m >= stop for stop in ready_at)
    )
    down = up_count - DOWN_LAG

    @pl.when(core == 0)
    def _():
        send(("own",), up_at(z, 0), up_at(z, 0), pair)
        tok_forward(1, 0)
        tok_forward(-1, 0)

        @pl.when(permutes)
        def _():
            send(("perm",), stage, perm_dst, perm_peer)

        tok_forward(1, 2)
        tok_forward(-1, 2)
        with jax.named_scope("tokown"):
            message(("own",), tok_own(1), tok_own(1), pair).wait_recv()
        for m in (1, 3):
            tok_forward(1, m)
            tok_forward(-1, m)
        for m in range(tok_count):
            tok_step(m)
        with jax.named_scope("uppair"):
            wait_bytes(
                recv_sem.at[number[("uppair", 0)]], up_all.at[pl.ds(0, (2 * n_z - 1) * up_rows), :]
            )

    @pl.when(core == 1)
    def _():
        send(("own",), tok_own(1), tok_own(1), pair)

        @pl.when(jnp.logical_and(moves, permutes))
        def _():
            send(("perm",), stage, perm_dst, perm_peer)

        for way in WAYS:
            for m in range(WEIGHT_CHUNKS):
                if chunk_of(way, m, WEIGHT_CHUNKS) == 1:
                    up_forward(way, m)
        send(("uppair", 0), up_at(z, 1), up_at(z, 1), pair)
        with jax.named_scope("upown"):
            message(("own",), up_at(z, 0), up_at(z, 0), pair).wait_recv()
        for way in WAYS:
            for m in range(WEIGHT_CHUNKS):
                if chunk_of(way, m, WEIGHT_CHUNKS) == 0:
                    up_forward(way, m)
        for tick in range(up_count):
            up_step(tick)
            if tick == DOWN_LAG - 1:
                with jax.named_scope("perm"):
                    mine, other = dn_at(z, odd), dn_at(z, 1 - odd)

                    @pl.when(jnp.logical_or(moves, jnp.logical_not(permutes)))
                    def _():
                        message(("perm",), mine, mine, perm_peer).wait_recv()

                    send(("across",), mine, mine, across)
                    message(("across",), other, other, across).wait_recv()

                for m in range(WEIGHT_CHUNKS):
                    for way in WAYS:
                        dn_forward(way, m)
                for c in range(WEIGHT_CHUNKS):
                    send(("dnpair", 0), dn_at(z, c), dn_at(z, c), pair)
            dn_step(tick - DOWN_LAG)
        with jax.named_scope("tokpair"):
            wait_bytes(recv_sem.at[number[("tokpair", 0)]], tok_all.at[pl.ds(0, (n_x - 1) * rows), :])

    pieces = 4
    piece = all_rows // pieces
    for p in range(pieces):
        with jax.named_scope(f"hid{p}"):
            own = pl.ds(pl.multiple_of(core * all_rows + p * piece, piece), piece)
            product = jnp.dot(tok_all[own, :], up_all[...], preferred_element_type=F32)
            rectified = jnp.maximum(product, 0.0)
            hid[pl.ds(p * piece, piece), :] = (rectified * rectified).astype(BF16)

    near = 2 * (lax.rem(z, QUARTERS) // 2) - 1
    own_quarter = z // QUARTERS
    quarter = [lax.rem(own_quarter + QUARTERS + shift, QUARTERS) for shift in (0, near, -near, 2)]

    def columns(j):
        return pl.ds(pl.multiple_of(quarter[j] * q_cols, q_cols), q_cols)

    def rs_rows(xx):
        return pl.ds(pl.multiple_of(xx * rows, rows), rows)

    def send_rs(way, j, k):
        where = slot[(way, j, k)]
        total = part[j, rs_rows(lax.rem(x + way * k + n_x, n_x)), :]
        if k < chain_start(j, way, half_x):
            before = slot[(way, j, k + 1)]
            message(("rs", way, j, k + 1), rs_out.at[before], rs_in.at[before], x_peer[way]).wait_recv()
            total = total + rs_in[before].astype(F32)
        rs_out[where] = total.astype(BF16)
        send(("rs", way, j, k), rs_out.at[where], rs_in.at[where], x_peer[way])

    def begin(j):
        @pl.when(core == 0)
        def _():
            shards = 2 * (ready_at[j] - (ready_at[j - 1] if j else 0)) + (WEIGHT_CHUNKS if j == 0 else 0)
            with jax.named_scope(f"dnpair{j}"):
                wait_bytes(
                    recv_sem.at[number[("dnpair", j)]],
                    dn_all.at[pl.ds(0, shards * dn_rows * dn_cols // d), :],
                )

        with jax.named_scope(f"part{j}"):
            part[j] = jnp.dot(hid[...], dn_all[:, columns(j)], preferred_element_type=F32)
        for way in WAYS:
            send_rs(way, j, chain_start(j, way, half_x))

    def go_on(j, later):
        with jax.named_scope(f"rs{j}r{later}"):
            for way in WAYS:
                k = chain_start(j, way, half_x) - later
                if k >= 1:
                    send_rs(way, j, k)

    def end(j):
        with jax.named_scope(f"end{j}"):
            total = part[j, rs_rows(x), :]
            for way in WAYS:
                here = slot[(way, j, 1)]
                message(("rs", way, j, 1), rs_out.at[here], rs_in.at[here], x_peer[way]).wait_recv()
                total = total + rs_in[here].astype(F32)
            y_out[:, columns(j)] = total.astype(BF16)

    def more_down(stop):
        nonlocal down
        steps = range(down, stop)
        down = max(down, stop)
        if steps:

            @pl.when(core == 1)
            def _():
                for m in steps:
                    dn_step(m)

    more_down(ready_at[0])
    begin(0)
    more_down(ready_at[1])
    begin(1)
    more_down(ready_at[1] + 2)
    go_on(0, 1)
    more_down(ready_at[2])
    begin(2)
    more_down(ready_at[3])
    begin(3)
    for j in range(1, QUARTERS):
        go_on(j, 1)
    for later in range(2, half_x):
        for j in range(QUARTERS):
            go_on(j, later)
    for j in range(QUARTERS):
        end(j)

    with jax.named_scope("drain"):

        def sent(kind, ref):
            wait_bytes(send_sem.at[SEND_SEMS.index(kind)], ref)

        sent("rs", rs_out)

        @pl.when(core == 0)
        def _():
            sent("own", up_at(z, 0))

            @pl.when(permutes)
            def _():
                sent("perm", stage)

            sent("tok", tok_all.at[pl.ds(0, 2 * tok_count * (rows // 2)), :])
            sent("tokpair", tok_all.at[pl.ds(0, (n_x - 1) * rows), :])

        @pl.when(core == 1)
        def _():
            sent("own", tok_own(1))

            @pl.when(jnp.logical_and(moves, permutes))
            def _():
                sent("perm", stage)

            sent("across", stage)
            sent("up", up_all.at[pl.ds(0, 2 * up_count * up_rows), :])
            sent("uppair", up_all.at[pl.ds(0, (2 * n_z - 1) * up_rows), :])
            sent("dn", dn_all.at[pl.ds(0, 2 * dn_count * dn_rows * dn_cols // d), :])
            sent("dnpair", dn_all)


def copier(*refs):
    count = len(refs) // 2
    sem = refs[-1]
    copies = [
        pltpu.make_async_copy(refs[k], refs[count + k], sem.at[k]) for k in range(count)
    ]
    for copy in copies:
        copy.start()
    for copy in copies:
        copy.wait()


def solution(mesh):
    n_f, n_x = mesh.shape["fs"], mesh.shape["tp"]
    assert n_f == 4 * n_x and n_x == 8 and mesh.shape["grp"] % 2 == 0
    number = receive_numbers(n_f // 2, n_x)
    slots = [name[1:] for name in number if name[0] == "rs"]
    slot = {name: k for k, name in enumerate(slots)}

    def on_device(tokens, up_master, down_master, norm_gain):
        rows, d = tokens.shape
        up_rows, width = up_master.shape
        dn_rows, dn_cols = down_master.shape
        results = (
            jax.ShapeDtypeStruct((up_rows * n_f, width), BF16),
            jax.ShapeDtypeStruct((width, d), BF16),
            jax.ShapeDtypeStruct((rows, d), BF16),
        )
        in_hbm = pl.BlockSpec(memory_space=pltpu.HBM)
        in_vmem = pl.BlockSpec(memory_space=pltpu.VMEM)
        arrays = (tokens, up_master, down_master, norm_gain.reshape(1, up_rows))
        made = pl.pallas_call(
            functools.partial(kernel, number, slot, n_f, n_x),
            out_shape=results,
            in_specs=[in_hbm] * 4,
            out_specs=(in_vmem,) * 3,
            scratch_shapes=[
                pltpu.VMEM((rows, d), BF16),
                pltpu.VMEM((up_rows, width), F32),
                pltpu.VMEM((dn_rows, dn_cols), F32),
                pltpu.VMEM((1, up_rows), F32),
                pltpu.VMEM((dn_rows, dn_cols), BF16),
                pltpu.VMEM((2 * n_x * rows, d), BF16),
                pltpu.VMEM((n_x * rows, width), BF16),
                pltpu.VMEM((QUARTERS, n_x * rows, d // QUARTERS), F32),
                pltpu.VMEM((len(slots), rows, d // QUARTERS), BF16),
                pltpu.VMEM((len(slots), rows, d // QUARTERS), BF16),
                pltpu.SemaphoreType.DMA((len(SEND_SEMS),)),
                pltpu.SemaphoreType.DMA((len(number),)),
                pltpu.SemaphoreType.DMA((4,)),
            ],
            compiler_params=pltpu.CompilerParams(
                collective_id=0, has_side_effects=True, vmem_limit_bytes=32 * 1024 * 1024
            ),
            name="handoff",
        )(*(pltpu.with_memory_space_constraint(a, pltpu.HBM) for a in arrays))
        return pl.pallas_call(
            copier,
            out_shape=results,
            in_specs=[in_vmem] * 3,
            out_specs=(in_hbm,) * 3,
            scratch_shapes=[pltpu.SemaphoreType.DMA((3,))],
            compiler_params=pltpu.CompilerParams(vmem_limit_bytes=16 * 1024 * 1024),
            name="hand_out",
        )(*made)

    in_specs = (P(("grp", "fs", "tp"), None), P("fs", "tp"), P("fs", "tp"), P("fs"))
    out_specs = (P("grp", "tp"), P(("grp", "tp"), None), P(("grp", "fs", "tp"), None))
    return jax.shard_map(on_device, mesh=mesh, in_specs=in_specs, out_specs=out_specs, check_vma=False)
```

```python
import functools

import jax
import jax.numpy as jnp
from jax import lax
from jax.experimental import pallas as pl
from jax.experimental.pallas import tpu as pltpu
from jax.sharding import PartitionSpec as P

MESH = pl.DeviceIdType.MESH
BF16 = jnp.bfloat16
F32 = jnp.float32
QUARTERS = 4
DOWN_LAG = 8
TOK_CHUNKS = 4
WEIGHT_CHUNKS = 2
WAYS = (1, -1)
SEND_SEMS = ("own", "perm", "across", "tok", "tokpair", "up", "uppair", "upacross", "dn", "dnpair", "dnacross", "rs")


def ring_messages(n, chunks):
    return (n // 2 - 1) * chunks + chunks // 2


def chunk_of(way, m, chunks):
    return (m + (0 if way == 1 else chunks // 2)) % chunks


def chain_start(j, way, half_x):
    return half_x if (j % 2 == 0) == (way == 1) else half_x - 1


def receive_numbers(n_z, n_x):
    names = [("own",), ("perm",), ("across",), ("tokpair", 0), ("uppair", 0)]
    names += [("dnpair", group) for group in range(QUARTERS)]
    names += [(kind + "across", away) for kind in ("up", "dn") for away in range(n_z // 2)]
    names += [("tok", way, m) for way in WAYS for m in range(ring_messages(n_x, TOK_CHUNKS))]
    for kind in ("up", "dn"):
        names += [(kind, way, m) for way in WAYS for m in range(ring_messages(n_z, WEIGHT_CHUNKS))]
    names += [
        ("rs", way, j, k)
        for way in WAYS
        for j in range(QUARTERS)
        for k in range(chain_start(j, way, n_x // 2), 0, -1)
    ]
    return {name: number for number, name in enumerate(names)}


def kernel(
    number, slot, n_f, n_x,
    tok_in, up_in, dn_in, gain_in,
    up_all, dn_all, y_out,
    tok_v, up_v, dn_v, gain_v, stage, tok_all, hid, part, rs_out, rs_in,
    send_sem, recv_sem, load_sem,
):
    x = lax.axis_index("tp")
    f = lax.axis_index("fs")
    z, core = f // 2, f % 2
    n_z, half_x = n_f // 2, n_x // 2
    rows, d = tok_in.shape
    up_rows, width = up_in.shape
    dn_rows, dn_cols = dn_in.shape
    q_cols = d // QUARTERS
    all_rows = n_x * rows

    group = lax.axis_index("grp")
    odd = group % 2

    def at(**where):
        return {"grp": group, "fs": f, "tp": x} | where

    x_peer = {way: at(tp=lax.rem(x + way + n_x, n_x)) for way in WAYS}
    z_peer = {way: at(fs=lax.rem(f + 2 * way + n_f, n_f)) for way in WAYS}
    pair = at(fs=2 * z + 1 - core)
    z_hi, z_lo = z // 2, z % 2
    perm_chip = 2 * x + z_lo
    perm_peer = at(tp=z_hi, fs=perm_chip * 2 + 1)
    stays = z_hi == x
    moves = jnp.logical_not(stays)
    permutes = core == odd
    across = at(grp=group + 1 - 2 * odd)

    def greet(peer):
        pl.semaphore_signal(barrier, inc=1, device_id=peer, device_id_type=MESH)

    barrier = pltpu.get_barrier_semaphore()
    for peer in (x_peer[1], x_peer[-1], pair):
        greet(peer)

    @pl.when(core == 1)
    def _():
        for way in WAYS:
            greet(z_peer[way])
        greet(across)

        @pl.when(moves)
        def _():
            greet(at(tp=z_hi, fs=perm_chip * 2 + odd))

    loads = [
        pltpu.make_async_copy(src, dst, load_sem.at[k])
        for k, (src, dst) in enumerate(((dn_in, dn_v), (tok_in, tok_v), (gain_in, gain_v), (up_in, up_v)))
    ]
    for load in loads:
        load.start()

    def up_at(zz, c):
        return up_all.at[pl.ds(pl.multiple_of((zz * 2 + c) * up_rows, up_rows), up_rows), :]

    def up_part(zz, c):
        size = up_rows // WEIGHT_CHUNKS
        return up_all.at[pl.ds(pl.multiple_of((zz * 2 + odd) * up_rows + c * size, size), size), :]

    def dn_at(zz, c):
        row = pl.multiple_of((lax.rem(zz, 2) * 2 + c) * dn_rows, dn_rows)
        col = pl.multiple_of((zz // 2) * dn_cols, dn_cols)
        return dn_all.at[pl.ds(row, dn_rows), pl.ds(col, dn_cols)]

    def dn_part(zz, c):
        size = dn_rows // WEIGHT_CHUNKS
        row = pl.multiple_of((lax.rem(zz, 2) * 2 + odd) * dn_rows + c * size, size)
        col = pl.multiple_of((zz // 2) * dn_cols, dn_cols)
        return dn_all.at[pl.ds(row, size), pl.ds(col, dn_cols)]

    def tok_at(xx, c):
        size = rows // 2
        row = pl.multiple_of((c % 2) * all_rows + xx * rows + (c // 2) * size, size)
        return tok_all.at[pl.ds(row, size), :]

    def tok_own(c):
        return tok_all.at[pl.ds(pl.multiple_of(c * all_rows + x * rows, rows), rows), :]

    def message(name, src, dst, peer):
        return pltpu.make_async_remote_copy(
            src_ref=src,
            dst_ref=dst,
            send_sem=send_sem.at[SEND_SEMS.index(name[0])],
            recv_sem=recv_sem.at[number[name]],
            device_id=peer,
            device_id_type=MESH,
        )

    def send(name, src, dst, peer):
        message(name, src, dst, peer).start()

    def wait_bytes(sem, ref):
        pltpu.make_async_copy(ref, ref, sem).wait()

    with jax.named_scope("own"):
        loads[1].wait()
        tokens = tok_v[...].astype(F32)
        scale = lax.rsqrt(jnp.mean(tokens * tokens, axis=-1, keepdims=True) + 1e-06)
        tok_own(core)[...] = (tokens * scale).astype(BF16)
        loads[0].wait()
        stage[...] = dn_v[...].astype(BF16)
        perm_dst = dn_all.at[
            pl.ds(pl.multiple_of((z_lo * 2 + core) * dn_rows, dn_rows), dn_rows),
            pl.ds(pl.multiple_of(x * dn_cols, dn_cols), dn_cols),
        ]

        @pl.when(jnp.logical_and(stays, jnp.logical_and(permutes, core == 1)))
        def _():
            perm_dst[...] = stage[...]

        loads[2].wait()
        loads[3].wait()
        square = (up_rows, up_rows)
        diagonal = lax.broadcasted_iota(jnp.int32, square, 0) == lax.broadcasted_iota(jnp.int32, square, 1)
        gain = jnp.sum(jnp.where(diagonal, jnp.broadcast_to(gain_v[...], square), 0.0), axis=1, keepdims=True)
        up_at(z, core)[...] = (gain * up_v[...]).astype(BF16)

    with jax.named_scope("barrier"):
        pl.semaphore_wait(barrier, 3 + 3 * core + jnp.where(jnp.logical_and(moves, permutes), 1, 0))

    def stream(kind, n, chunks, me, place, peers, onward):
        count = ring_messages(n, chunks)

        def block(way, m, away):
            owner = lax.rem(me - way * (m // chunks + away) + n, n)
            return place(owner, chunk_of(way, m, chunks))

        def forward(way, m):
            if m < count:
                ref = block(way, m, 0)
                send((kind, way, m), ref, ref, peers[way])

        def step(m):
            if 0 <= m < count:
                with jax.named_scope(f"{kind}{m}"):
                    for way in WAYS:
                        ref = block(way, m, 1)
                        message((kind, way, m), ref, ref, peers[way]).wait_recv()
                        forward(way, m + chunks)
                        for name, peer in onward(way, m):
                            send(name, ref, ref, peer)

        return count, forward, step

    last = ring_messages(n_z, WEIGHT_CHUNKS)
    ready_at = [distance * WEIGHT_CHUNKS for distance in (3, 5, 7)] + [last]

    def quarter_of(m):
        return sum(m >= stop for stop in ready_at)

    tok_count, tok_forward, tok_step = stream(
        "tok", n_x, TOK_CHUNKS, x, tok_at, x_peer,
        lambda way, m: [(("tokpair", 0), pair)] if chunk_of(way, m, TOK_CHUNKS) % 2 else [],
    )
    up_count, up_forward, up_step = stream(
        "up", n_z, WEIGHT_CHUNKS, z, up_part, z_peer,
        lambda way, m: [(("uppair", 0), pair), (("upacross", m // WEIGHT_CHUNKS), across)],
    )
    dn_count, dn_forward, dn_step = stream(
        "dn", n_z, WEIGHT_CHUNKS, z, dn_part, z_peer,
        lambda way, m: [(("dnpair", quarter_of(m)), pair), (("dnacross", m // WEIGHT_CHUNKS), across)],
    )

    def from_across(kind, away, place, whole, group):
        with jax.named_scope(f"{kind}across{away}"):
            chips = (1, -1) if away < n_z // 2 - 1 else (1,)
            wait_bytes(
                recv_sem.at[number[(kind + "across", away)]],
                whole.at[pl.ds(0, len(chips) * up_rows * width // whole.shape[1]), :],
            )
            for way in chips:
                ref = place(lax.rem(z - way * (away + 1) + n_z, n_z), 1 - odd)
                send((kind + "pair", group), ref, ref, pair)

    def up_across(away):
        from_across("up", away, up_at, up_all, 0)

    def dn_across(away):
        if 0 <= away:
            from_across("dn", away, dn_at, dn_all, quarter_of(away * WEIGHT_CHUNKS))

    @pl.when(core == 0)
    def _():
        @pl.when(permutes)
        def _():
            send(("perm",), stage, perm_dst, perm_peer)

        send(("own",), up_at(z, 0), up_at(z, 0), pair)
        tok_forward(1, 0)
        tok_forward(-1, 0)
        tok_forward(1, 2)
        tok_forward(-1, 2)
        with jax.named_scope("tokown"):
            message(("own",), tok_own(1), tok_own(1), pair).wait_recv()
        for m in (1, 3):
            tok_forward(1, m)
            tok_forward(-1, m)
        for m in range(tok_count):
            tok_step(m)
        with jax.named_scope("uppair"):
            wait_bytes(
                recv_sem.at[number[("uppair", 0)]], up_all.at[pl.ds(0, (2 * n_z - 1) * up_rows), :]
            )

    @pl.when(core == 1)
    def _():
        @pl.when(jnp.logical_and(moves, permutes))
        def _():
            send(("perm",), stage, perm_dst, perm_peer)

        send(("own",), tok_own(1), tok_own(1), pair)

        def up_first():
            for m in range(WEIGHT_CHUNKS):
                for way in WAYS:
                    up_forward(way, m)

        @pl.when(odd == 1)
        def _():
            up_first()

        send(("uppair", 0), up_at(z, 1), up_at(z, 1), pair)
        with jax.named_scope("upown"):
            message(("own",), up_at(z, 0), up_at(z, 0), pair).wait_recv()

        @pl.when(odd == 0)
        def _():
            up_first()

        mine, other = dn_at(z, odd), dn_at(z, 1 - odd)
        for tick in range(up_count):
            up_step(tick)
            if tick == DOWN_LAG - 1:
                with jax.named_scope("perm"):

                    @pl.when(jnp.logical_or(moves, jnp.logical_not(permutes)))
                    def _():
                        message(("perm",), mine, mine, perm_peer).wait_recv()

                for m in range(WEIGHT_CHUNKS):
                    for way in WAYS:
                        dn_forward(way, m)
                send(("across",), mine, mine, across)
                send(("dnpair", 0), mine, mine, pair)
            dn_step(tick - DOWN_LAG)
            if tick % WEIGHT_CHUNKS and tick > WEIGHT_CHUNKS:
                up_across(tick // WEIGHT_CHUNKS - 1)
                dn_across((tick - DOWN_LAG) // WEIGHT_CHUNKS - 1)
        with jax.named_scope("across"):
            message(("across",), other, other, across).wait_recv()
        send(("dnpair", 0), other, other, pair)
        up_across(n_z // 2 - 2)
        dn_step(up_count - DOWN_LAG)
        up_across(n_z // 2 - 1)
        dn_across(2)
        with jax.named_scope("tokpair"):
            wait_bytes(recv_sem.at[number[("tokpair", 0)]], tok_all.at[pl.ds(0, (n_x - 1) * rows), :])

    down = up_count - DOWN_LAG + 1
    down_across = 3

    def more_down(stop, stop_across):
        nonlocal down, down_across
        steps, groups = range(down, stop), range(down_across, stop_across)
        down, down_across = max(down, stop), max(down_across, stop_across)
        if steps or groups:

            @pl.when(core == 1)
            def _():
                for m in steps:
                    dn_step(m)
                for away in groups:
                    dn_across(away)

    pieces = 4
    piece = all_rows // pieces
    for p in range(pieces):
        with jax.named_scope(f"hid{p}"):
            own = pl.ds(pl.multiple_of(core * all_rows + p * piece, piece), piece)
            product = jnp.dot(tok_all[own, :], up_all[...], preferred_element_type=F32)
            rectified = jnp.maximum(product, 0.0)
            hid[pl.ds(p * piece, piece), :] = (rectified * rectified).astype(BF16)
        if p < pieces - 1:
            more_down(down + 1, 4 if p == 1 else 0)

    near = 2 * (lax.rem(z, QUARTERS) // 2) - 1
    own_quarter = z // QUARTERS
    quarter = [lax.rem(own_quarter + QUARTERS + shift, QUARTERS) for shift in (0, near, -near, 2)]

    def columns(j):
        return pl.ds(pl.multiple_of(quarter[j] * q_cols, q_cols), q_cols)

    def rs_rows(xx):
        return pl.ds(pl.multiple_of(xx * rows, rows), rows)

    def send_rs(way, j, k):
        where = slot[(way, j, k)]
        total = part[j, rs_rows(lax.rem(x + way * k + n_x, n_x)), :]
        if k < chain_start(j, way, half_x):
            before = slot[(way, j, k + 1)]
            message(("rs", way, j, k + 1), rs_out.at[before], rs_in.at[before], x_peer[way]).wait_recv()
            total = total + rs_in[before].astype(F32)
        rs_out[where] = total.astype(BF16)
        send(("rs", way, j, k), rs_out.at[where], rs_in.at[where], x_peer[way])

    def begin(j):
        @pl.when(core == 0)
        def _():
            shards = 2 * (ready_at[j] - (ready_at[j - 1] if j else 0)) + (WEIGHT_CHUNKS if j == 0 else 0)
            with jax.named_scope(f"dnpair{j}"):
                wait_bytes(
                    recv_sem.at[number[("dnpair", j)]],
                    dn_all.at[pl.ds(0, shards * dn_rows * dn_cols // d), :],
                )

        with jax.named_scope(f"part{j}"):
            part[j] = jnp.dot(hid[...], dn_all[:, columns(j)], preferred_element_type=F32)
        for way in WAYS:
            send_rs(way, j, chain_start(j, way, half_x))

    def go_on(j, later):
        with jax.named_scope(f"rs{j}r{later}"):
            for way in WAYS:
                k = chain_start(j, way, half_x) - later
                if k >= 1:
                    send_rs(way, j, k)

    def end(j):
        with jax.named_scope(f"end{j}"):
            total = part[j, rs_rows(x), :]
            for way in WAYS:
                here = slot[(way, j, 1)]
                message(("rs", way, j, 1), rs_out.at[here], rs_in.at[here], x_peer[way]).wait_recv()
                total = total + rs_in[here].astype(F32)
            y_out[:, columns(j)] = total.astype(BF16)

    begin(0)
    more_down(12, 5)
    begin(1)
    more_down(13, 5)
    go_on(0, 1)
    more_down(14, 6)
    more_down(15, 6)
    go_on(1, 1)
    more_down(15, 7)
    begin(2)
    more_down(15, 8)
    begin(3)
    for j, later in ((0, 2), (2, 1), (3, 1), (1, 2), (2, 2), (0, 3), (3, 2), (1, 3), (2, 3), (3, 3)):
        go_on(j, later)
    for j in range(QUARTERS):
        end(j)

    with jax.named_scope("drain"):

        def sent(kind, ref):
            wait_bytes(send_sem.at[SEND_SEMS.index(kind)], ref)

        sent("rs", rs_out)

        @pl.when(core == 0)
        def _():
            sent("own", up_at(z, 0))

            @pl.when(permutes)
            def _():
                sent("perm", stage)

            sent("tok", tok_all.at[pl.ds(0, 2 * tok_count * (rows // 2)), :])
            sent("tokpair", tok_all.at[pl.ds(0, (n_x - 1) * rows), :])

        @pl.when(core == 1)
        def _():
            sent("own", tok_own(1))

            @pl.when(jnp.logical_and(moves, permutes))
            def _():
                sent("perm", stage)

            sent("across", stage)
            for kind in ("up", "upacross"):
                sent(kind, up_all.at[pl.ds(0, 2 * up_count * (up_rows // WEIGHT_CHUNKS)), :])
            sent("uppair", up_all.at[pl.ds(0, (2 * n_z - 1) * up_rows), :])
            for kind in ("dn", "dnacross"):
                sent(kind, dn_all.at[pl.ds(0, 2 * dn_count * dn_rows * dn_cols // (WEIGHT_CHUNKS * d)), :])
            sent("dnpair", dn_all)


def copier(*refs):
    count = len(refs) // 2
    sem = refs[-1]
    copies = [
        pltpu.make_async_copy(refs[k], refs[count + k], sem.at[k]) for k in range(count)
    ]
    for copy in copies:
        copy.start()
    for copy in copies:
        copy.wait()


def solution(mesh):
    n_f, n_x = mesh.shape["fs"], mesh.shape["tp"]
    assert n_f == 4 * n_x and n_x == 8 and mesh.shape["grp"] % 2 == 0
    number = receive_numbers(n_f // 2, n_x)
    slots = [name[1:] for name in number if name[0] == "rs"]
    slot = {name: k for k, name in enumerate(slots)}

    def on_device(tokens, up_master, down_master, norm_gain):
        rows, d = tokens.shape
        up_rows, width = up_master.shape
        dn_rows, dn_cols = down_master.shape
        results = (
            jax.ShapeDtypeStruct((up_rows * n_f, width), BF16),
            jax.ShapeDtypeStruct((width, d), BF16),
            jax.ShapeDtypeStruct((rows, d), BF16),
        )
        in_hbm = pl.BlockSpec(memory_space=pltpu.HBM)
        in_vmem = pl.BlockSpec(memory_space=pltpu.VMEM)
        arrays = (tokens, up_master, down_master, norm_gain.reshape(1, up_rows))
        made = pl.pallas_call(
            functools.partial(kernel, number, slot, n_f, n_x),
            out_shape=results,
            in_specs=[in_hbm] * 4,
            out_specs=(in_vmem,) * 3,
            scratch_shapes=[
                pltpu.VMEM((rows, d), BF16),
                pltpu.VMEM((up_rows, width), F32),
                pltpu.VMEM((dn_rows, dn_cols), F32),
                pltpu.VMEM((1, up_rows), F32),
                pltpu.VMEM((dn_rows, dn_cols), BF16),
                pltpu.VMEM((2 * n_x * rows, d), BF16),
                pltpu.VMEM((n_x * rows, width), BF16),
                pltpu.VMEM((QUARTERS, n_x * rows, d // QUARTERS), F32),
                pltpu.VMEM((len(slots), rows, d // QUARTERS), BF16),
                pltpu.VMEM((len(slots), rows, d // QUARTERS), BF16),
                pltpu.SemaphoreType.DMA((len(SEND_SEMS),)),
                pltpu.SemaphoreType.DMA((len(number),)),
                pltpu.SemaphoreType.DMA((4,)),
            ],
            compiler_params=pltpu.CompilerParams(
                collective_id=0, has_side_effects=True, vmem_limit_bytes=32 * 1024 * 1024
            ),
            name="handoff",
        )(*(pltpu.with_memory_space_constraint(a, pltpu.HBM) for a in arrays))
        return pl.pallas_call(
            copier,
            out_shape=results,
            in_specs=[in_vmem] * 3,
            out_specs=(in_hbm,) * 3,
            scratch_shapes=[pltpu.SemaphoreType.DMA((3,))],
            compiler_params=pltpu.CompilerParams(vmem_limit_bytes=16 * 1024 * 1024),
            name="hand_out",
        )(*made)

    in_specs = (P(("grp", "fs", "tp"), None), P("fs", "tp"), P("fs", "tp"), P("fs"))
    out_specs = (P("grp", "tp"), P(("grp", "tp"), None), P(("grp", "fs", "tp"), None))
    return jax.shard_map(on_device, mesh=mesh, in_specs=in_specs, out_specs=out_specs, check_vma=False)
```

```python
import functools

import jax
import jax.numpy as jnp
from jax import lax
from jax.experimental import pallas as pl
from jax.experimental.pallas import tpu as pltpu
from jax.sharding import PartitionSpec as P

MESH = pl.DeviceIdType.MESH
BF16 = jnp.bfloat16
F32 = jnp.float32
QUARTERS = 4
TOK_CHUNKS = 4
WEIGHT_CHUNKS = 2
WAYS = (1, -1)
REACH = (3, 5, 7, 8)
SEND_SEMS = ("own", "perm", "relay", "pass", "tok", "tokpair", "up", "uppair", "upacross", "dn", "dnpair", "dnacross", "rs")


def ring_messages(n, chunks):
    return (n // 2 - 1) * chunks + chunks // 2


def chunk_of(way, m, chunks):
    return (m + (0 if way == 1 else chunks // 2)) % chunks


def chain_start(j, way, half_x):
    return half_x if (j % 2 == 0) == (way == 1) else half_x - 1


def limit(way, c, half_z):
    return half_z if (c == 0) == (way == 1) else half_z - 1


def quarter_from(far):
    return sum(far > reach for reach in REACH[:-1])


def receive_numbers(n_z, n_x):
    half_z, half_x = n_z // 2, n_x // 2
    both = [("own",), ("uppair", 0)] + [("dnpair", quarter) for quarter in range(QUARTERS)]
    both += [
        ("rs", way, j, k) for way in WAYS for j in range(QUARTERS) for k in range(chain_start(j, way, half_x), 0, -1)
    ]
    core_0 = [("upacross", 0)] + [("dnacross", quarter) for quarter in range(QUARTERS)]
    core_0 += [("tok", way, m) for way in WAYS for m in range(ring_messages(n_x, TOK_CHUNKS))]
    core_1 = [("perm",), ("relay",), ("tokpair",)]
    for kind in ("up", "dn"):
        core_1 += [
            (kind, way, far, c)
            for way in WAYS
            for c in range(WEIGHT_CHUNKS)
            for far in range(1, limit(way, c, half_z) + 1)
        ]
    number = {name: k for k, name in enumerate(both)}
    for names in (core_0, core_1):
        number |= {name: len(both) + k for k, name in enumerate(names)}
    return number


def kernel(
    number, slot, n_f, n_x,
    tok_in, up_in, dn_in, gain_in,
    up_all, dn_all, y_out,
    tok_v, up_v, dn_v, gain_v, stage, relay, tok_all, hid, part, rs_out, rs_in,
    send_sem, recv_sem, load_sem,
):
    x = lax.axis_index("tp")
    f = lax.axis_index("fs")
    z, core = f // 2, f % 2
    n_z, half_x = n_f // 2, n_x // 2
    rows, d = tok_in.shape
    up_rows, width = up_in.shape
    dn_rows, dn_cols = dn_in.shape
    q_cols = d // QUARTERS
    all_rows = n_x * rows

    group = lax.axis_index("grp")
    odd = group % 2

    def at(**where):
        return {"grp": group, "fs": f, "tp": x} | where

    x_peer = {way: at(tp=lax.rem(x + way + n_x, n_x)) for way in WAYS}
    z_peer = {hop: at(fs=lax.rem(f + 2 * hop + n_f, n_f)) for hop in (1, -1, 2, -2)}
    pair = at(fs=2 * z + 1 - core)
    z_hi, z_lo = z // 2, z % 2
    to_plane = lax.rem(x + half_x, n_x)
    relays = to_plane == n_x - 1
    perm_peer = at(tp=z_hi, fs=lax.rem(2 * to_plane + z_lo + 2 * (to_plane // (n_x - 1)), n_z) * 2 + 1)
    perm_source = at(tp=lax.rem(z_hi + half_x, n_x), fs=(2 * x + z_lo) * 2 + odd)
    relay_source = at(tp=lax.rem(n_x - 1 + half_x, n_x), fs=(2 * x + z_lo) * 2 + odd)
    first_planes, last_planes = z_hi == 0, z_hi == n_x - 1
    permutes = core == odd
    across = [at(grp=group + 1 - 2 * odd, fs=2 * z + c) for c in range(2)]

    def greet(peer):
        pl.semaphore_signal(barrier, inc=1, device_id=peer, device_id_type=MESH)

    barrier = pltpu.get_barrier_semaphore()
    for peer in (x_peer[1], x_peer[-1], pair):
        greet(peer)

    @pl.when(core == 0)
    def _():
        greet(across[1])

    @pl.when(core == 1)
    def _():
        for hop in z_peer:
            greet(z_peer[hop])

        @pl.when(jnp.logical_not(last_planes))
        def _():
            greet(perm_source)

        @pl.when(first_planes)
        def _():
            greet(relay_source)

    loads = [
        pltpu.make_async_copy(src, dst, load_sem.at[k])
        for k, (src, dst) in enumerate(((dn_in, dn_v), (tok_in, tok_v), (gain_in, gain_v), (up_in, up_v)))
    ]
    for load in loads:
        load.start()

    def up_at(zz, c):
        return up_all.at[pl.ds(pl.multiple_of((zz * 2 + c) * up_rows, up_rows), up_rows), :]

    def up_part(zz, c):
        size = up_rows // WEIGHT_CHUNKS
        return up_all.at[pl.ds(pl.multiple_of((zz * 2 + odd) * up_rows + c * size, size), size), :]

    def dn_at(zz, c):
        row = pl.multiple_of((lax.rem(zz, 2) * 2 + c) * dn_rows, dn_rows)
        col = pl.multiple_of(lax.rem(zz // 2 + half_x, n_x) * dn_cols, dn_cols)
        return dn_all.at[pl.ds(row, dn_rows), pl.ds(col, dn_cols)]

    def dn_part(zz, c):
        size = dn_rows // WEIGHT_CHUNKS
        row = pl.multiple_of((lax.rem(zz, 2) * 2 + odd) * dn_rows + c * size, size)
        col = pl.multiple_of(lax.rem(zz // 2 + half_x, n_x) * dn_cols, dn_cols)
        return dn_all.at[pl.ds(row, size), pl.ds(col, dn_cols)]

    def tok_at(xx, c):
        size = rows // 2
        row = pl.multiple_of((c % 2) * all_rows + xx * rows + (c // 2) * size, size)
        return tok_all.at[pl.ds(row, size), :]

    def tok_own(c):
        return tok_all.at[pl.ds(pl.multiple_of(c * all_rows + x * rows, rows), rows), :]

    def message(name, src, dst, peer, sem=None):
        return pltpu.make_async_remote_copy(
            src_ref=src,
            dst_ref=dst,
            send_sem=send_sem.at[SEND_SEMS.index(sem or name[0])],
            recv_sem=recv_sem.at[number[name]],
            device_id=peer,
            device_id_type=MESH,
        )

    def send(name, src, dst, peer, sem=None):
        message(name, src, dst, peer, sem).start()

    def wait_bytes(sem, ref):
        pltpu.make_async_copy(ref, ref, sem).wait()

    with jax.named_scope("own"):
        loads[1].wait()
        tokens = tok_v[...].astype(F32)
        scale = lax.rsqrt(jnp.mean(tokens * tokens, axis=-1, keepdims=True) + 1e-06)
        tok_own(core)[...] = (tokens * scale).astype(BF16)
        loads[0].wait()
        stage[...] = dn_v[...].astype(BF16)
        perm_dst = dn_all.at[
            pl.ds(pl.multiple_of((z_lo * 2 + core) * dn_rows, dn_rows), dn_rows),
            pl.ds(pl.multiple_of(x * dn_cols, dn_cols), dn_cols),
        ]
        loads[2].wait()
        loads[3].wait()
        square = (up_rows, up_rows)
        diagonal = lax.broadcasted_iota(jnp.int32, square, 0) == lax.broadcasted_iota(jnp.int32, square, 1)
        gain = jnp.sum(jnp.where(diagonal, jnp.broadcast_to(gain_v[...], square), 0.0), axis=1, keepdims=True)
        up_at(z, core)[...] = (gain * up_v[...]).astype(BF16)

    with jax.named_scope("barrier"):
        pl.semaphore_wait(barrier, 3 + 5 * core + jnp.where(permutes, 1, 0))

    def stream(kind, n, chunks, me, place, peers, onward):
        count = ring_messages(n, chunks)

        def block(way, m, away):
            owner = lax.rem(me - way * (m // chunks + away) + n, n)
            return place(owner, chunk_of(way, m, chunks))

        def forward(way, m):
            if m < count:
                ref = block(way, m, 0)
                send((kind, way, m), ref, ref, peers[way])

        def step(m):
            if 0 <= m < count:
                with jax.named_scope(f"{kind}{m}"):
                    for way in WAYS:
                        ref = block(way, m, 1)
                        message((kind, way, m), ref, ref, peers[way]).wait_recv()
                        forward(way, m + chunks)
                        for name, peer in onward(way, m):
                            send(name, ref, ref, peer)

        return count, forward, step

    tok_count, tok_forward, tok_step = stream(
        "tok", n_x, TOK_CHUNKS, x, tok_at, x_peer,
        lambda way, m: [(("tokpair",), pair)] if chunk_of(way, m, TOK_CHUNKS) % 2 else [],
    )

    half_z = n_z // 2
    weight_parts = [(way, c) for c in range(WEIGHT_CHUNKS) for way in WAYS]

    def weights(kind, part_at, block_at, whole, group_of):
        def part(way, c, far):
            return part_at(lax.rem(z - way * far + n_z, n_z), c)

        def launch(way, c, far):
            ref = part(way, c, far)
            for hop in (2, 1):
                if far + hop <= limit(way, c, half_z):
                    send((kind, way, far + hop, c), ref, ref, z_peer[way * hop])

        def first():
            for way, c in weight_parts:
                launch(way, c, 0)

        def step(far):
            parts = [(way, c) for way, c in weight_parts if far <= limit(way, c, half_z)]
            with jax.named_scope(f"{kind}{far}"):
                for way, c in parts:
                    ref = part(way, c, far)
                    message((kind, way, far, c), ref, ref, z_peer[way]).wait_recv()
                    if far % 2 == 0:
                        launch(way, c, far)
                for way, c in parts:
                    ref = part(way, c, far)
                    send((kind + "across", group_of(far)), ref, ref, across[0])
                    send((kind + "pair", group_of(far)), ref, ref, pair)

        def pass_on(group, start, stop, own=False):
            chips = [(way, far) for far in range(start, stop + 1) for way in (WAYS if far < half_z else (1,))]
            chips += [(1, 0)] if own else []
            with jax.named_scope(f"{kind}across{group}"):
                wait_bytes(
                    recv_sem.at[number[(kind + "across", group)]],
                    whole.at[pl.ds(0, len(chips) * up_rows * width // whole.shape[1]), :],
                )
                for way, far in chips:
                    ref = block_at(lax.rem(z - way * far + n_z, n_z), 1 - odd)
                    send((kind + "pair", group), ref, ref, pair)

        return first, step, pass_on

    up_first, up_step, up_pass_on = weights("up", up_part, up_at, up_all, lambda far: 0)
    dn_first, dn_step, dn_pass_on = weights("dn", dn_part, dn_at, dn_all, quarter_from)

    def permute():
        @pl.when(jnp.logical_and(permutes, jnp.logical_not(relays)))
        def _():
            send(("perm",), stage, perm_dst, perm_peer)

        @pl.when(jnp.logical_and(permutes, relays))
        def _():
            send(("relay",), stage, relay, perm_peer)

    @pl.when(core == 0)
    def _():
        permute()

        send(("own",), up_at(z, 0), up_at(z, 0), pair)
        tok_forward(1, 0)
        tok_forward(-1, 0)
        tok_forward(1, 2)
        tok_forward(-1, 2)
        with jax.named_scope("tokown"):
            message(("own",), tok_own(1), tok_own(1), pair).wait_recv()
        for m in (1, 3):
            tok_forward(1, m)
            tok_forward(-1, m)
        for m in range(tok_count):
            tok_step(m)
        up_pass_on(0, 1, half_z)
        dn_pass_on(0, 1, REACH[0], own=True)
        with jax.named_scope("uppair"):
            wait_bytes(recv_sem.at[number[("uppair", 0)]], up_all.at[pl.ds(0, n_z * up_rows), :])

    @pl.when(core == 1)
    def _():
        permute()

        send(("own",), tok_own(1), tok_own(1), pair)

        @pl.when(odd == 1)
        def _():
            up_first()

        send(("uppair", 0), up_at(z, 1), up_at(z, 1), pair)
        with jax.named_scope("upown"):
            message(("own",), up_at(z, 0), up_at(z, 0), pair).wait_recv()

        @pl.when(odd == 0)
        def _():
            up_first()

        mine = dn_at(z, odd)

        def relayed():
            @pl.when(first_planes)
            def _():
                with jax.named_scope("relay"):
                    message(("relay",), relay, relay, perm_peer).wait_recv()
                send(("perm",), relay, dn_at(lax.rem(z - 2 + n_z, n_z), odd), z_peer[-2], "pass")

        def permuted():
            with jax.named_scope("perm"):
                message(("perm",), mine, mine, perm_peer).wait_recv()
            dn_first()
            send(("dnacross", 0), mine, mine, across[0])
            send(("dnpair", 0), mine, mine, pair)

        def permuted_early():
            @pl.when(jnp.logical_not(last_planes))
            def _():
                permuted()

        def permuted_late():
            @pl.when(last_planes)
            def _():
                permuted()

        for act, *far in (
            (up_step, 2, 1, 4, 3), (relayed,), (permuted_early,), (up_step, 6, 5), (permuted_late,), (dn_step, 2, 1),
            (up_step, 8, 7), (dn_step, 4, 3, 6, 5, 8, 7),
        ):
            if far:
                for distance in far:
                    act(distance)
            else:
                act()
        with jax.named_scope("tokpair"):
            wait_bytes(recv_sem.at[number[("tokpair",)]], tok_all.at[pl.ds(0, (n_x - 1) * rows), :])
        with jax.named_scope("uppair"):
            wait_bytes(recv_sem.at[number[("uppair", 0)]], up_all.at[pl.ds(0, (n_z - 1) * up_rows), :])

    pieces = 4
    piece = all_rows // pieces
    for p in range(pieces):
        with jax.named_scope(f"hid{p}"):
            own = pl.ds(pl.multiple_of(core * all_rows + p * piece, piece), piece)
            product = jnp.dot(tok_all[own, :], up_all[...], preferred_element_type=F32)
            rectified = jnp.maximum(product, 0.0)
            hid[pl.ds(p * piece, piece), :] = (rectified * rectified).astype(BF16)

    near = 2 * (lax.rem(z, QUARTERS) // 2) - 1
    own_quarter = z // QUARTERS + 2
    quarter = [lax.rem(own_quarter + QUARTERS + shift, QUARTERS) for shift in (0, near, -near, 2)]

    def columns(j):
        return pl.ds(pl.multiple_of(quarter[j] * q_cols, q_cols), q_cols)

    def rs_rows(xx):
        return pl.ds(pl.multiple_of(xx * rows, rows), rows)

    def send_rs(way, j, k):
        where = slot[(way, j, k)]
        total = part[j, rs_rows(lax.rem(x + way * k + n_x, n_x)), :]
        if k < chain_start(j, way, half_x):
            before = slot[(way, j, k + 1)]
            message(("rs", way, j, k + 1), rs_out.at[before], rs_in.at[before], x_peer[way]).wait_recv()
            total = total + rs_in[before].astype(F32)
        rs_out[where] = total.astype(BF16)
        send(("rs", way, j, k), rs_out.at[where], rs_in.at[where], x_peer[way])

    def begin(j):
        if j:

            @pl.when(core == 0)
            def _():
                dn_pass_on(j, REACH[j - 1] + 1, REACH[j])

        chips = 2 * (REACH[j] - (REACH[j - 1] if j else 0)) + (j == 0) - (j == QUARTERS - 1)
        with jax.named_scope(f"dnpair{j}"):
            wait_bytes(recv_sem.at[number[("dnpair", j)]], dn_all.at[pl.ds(0, chips * dn_rows * dn_cols // d), :])
        with jax.named_scope(f"part{j}"):
            part[j] = jnp.dot(hid[...], dn_all[:, columns(j)], preferred_element_type=F32)
        for way in WAYS:
            send_rs(way, j, chain_start(j, way, half_x))

    def go_on(j, later):
        with jax.named_scope(f"rs{j}r{later}"):
            for way in WAYS:
                k = chain_start(j, way, half_x) - later
                if k >= 1:
                    send_rs(way, j, k)

    def end(j):
        with jax.named_scope(f"end{j}"):
            total = part[j, rs_rows(x), :]
            for way in WAYS:
                here = slot[(way, j, 1)]
                message(("rs", way, j, 1), rs_out.at[here], rs_in.at[here], x_peer[way]).wait_recv()
                total = total + rs_in[here].astype(F32)
            y_out[:, columns(j)] = total.astype(BF16)

    begin(0)
    begin(1)
    begin(2)
    go_on(0, 1)
    begin(3)
    for j in range(1, QUARTERS):
        go_on(j, 1)
    for later in range(2, half_x):
        for j in range(QUARTERS):
            go_on(j, later)
    for j in range(QUARTERS):
        end(j)

    with jax.named_scope("drain"):

        def sent(kind, ref):
            wait_bytes(send_sem.at[SEND_SEMS.index(kind)], ref)

        def permute_sent():
            @pl.when(jnp.logical_and(permutes, jnp.logical_not(relays)))
            def _():
                sent("perm", stage)

            @pl.when(jnp.logical_and(permutes, relays))
            def _():
                sent("relay", stage)

        sent("rs", rs_out)
        sent("dnpair", dn_all.at[pl.ds(0, n_z * dn_rows * dn_cols // d), :])

        @pl.when(core == 0)
        def _():
            sent("own", up_at(z, 0))

            permute_sent()

            sent("tok", tok_all.at[pl.ds(0, 2 * tok_count * (rows // 2)), :])
            sent("tokpair", tok_all.at[pl.ds(0, (n_x - 1) * rows), :])
            sent("uppair", up_all.at[pl.ds(0, (n_z - 1) * up_rows), :])

        @pl.when(core == 1)
        def _():
            sent("own", tok_own(1))

            permute_sent()

            @pl.when(first_planes)
            def _():
                sent("pass", stage)

            for kind in ("up", "upacross"):
                sent(kind, up_all.at[pl.ds(0, (n_z - 1) * up_rows), :])
            sent("uppair", up_all.at[pl.ds(0, n_z * up_rows), :])
            sent("dn", dn_all.at[pl.ds(0, (n_z - 1) * dn_rows * dn_cols // d), :])
            sent("dnacross", dn_all.at[pl.ds(0, n_z * dn_rows * dn_cols // d), :])


def copier(*refs):
    count = len(refs) // 2
    sem = refs[-1]
    copies = [
        pltpu.make_async_copy(refs[k], refs[count + k], sem.at[k]) for k in range(count)
    ]
    for copy in copies:
        copy.start()
    for copy in copies:
        copy.wait()


def solution(mesh):
    n_f, n_x = mesh.shape["fs"], mesh.shape["tp"]
    assert n_f == 4 * n_x and n_x == 8 and mesh.shape["grp"] % 2 == 0
    number = receive_numbers(n_f // 2, n_x)
    slots = [name[1:] for name in number if name[0] == "rs"]
    slot = {name: k for k, name in enumerate(slots)}

    def on_device(tokens, up_master, down_master, norm_gain):
        rows, d = tokens.shape
        up_rows, width = up_master.shape
        dn_rows, dn_cols = down_master.shape
        results = (
            jax.ShapeDtypeStruct((up_rows * n_f, width), BF16),
            jax.ShapeDtypeStruct((width, d), BF16),
            jax.ShapeDtypeStruct((rows, d), BF16),
        )
        in_hbm = pl.BlockSpec(memory_space=pltpu.HBM)
        in_vmem = pl.BlockSpec(memory_space=pltpu.VMEM)
        arrays = (tokens, up_master, down_master, norm_gain.reshape(1, up_rows))
        made = pl.pallas_call(
            functools.partial(kernel, number, slot, n_f, n_x),
            out_shape=results,
            in_specs=[in_hbm] * 4,
            out_specs=(in_vmem,) * 3,
            scratch_shapes=[
                pltpu.VMEM((rows, d), BF16),
                pltpu.VMEM((up_rows, width), F32),
                pltpu.VMEM((dn_rows, dn_cols), F32),
                pltpu.VMEM((1, up_rows), F32),
                pltpu.VMEM((dn_rows, dn_cols), BF16),
                pltpu.VMEM((dn_rows, dn_cols), BF16),
                pltpu.VMEM((2 * n_x * rows, d), BF16),
                pltpu.VMEM((n_x * rows, width), BF16),
                pltpu.VMEM((QUARTERS, n_x * rows, d // QUARTERS), F32),
                pltpu.VMEM((len(slots), rows, d // QUARTERS), BF16),
                pltpu.VMEM((len(slots), rows, d // QUARTERS), BF16),
                pltpu.SemaphoreType.DMA((len(SEND_SEMS),)),
                pltpu.SemaphoreType.DMA((max(number.values()) + 1,)),
                pltpu.SemaphoreType.DMA((4,)),
            ],
            compiler_params=pltpu.CompilerParams(
                collective_id=0, has_side_effects=True, vmem_limit_bytes=32 * 1024 * 1024
            ),
            name="handoff",
        )(*(pltpu.with_memory_space_constraint(a, pltpu.HBM) for a in arrays))
        return pl.pallas_call(
            copier,
            out_shape=results,
            in_specs=[in_vmem] * 3,
            out_specs=(in_hbm,) * 3,
            scratch_shapes=[pltpu.SemaphoreType.DMA((3,))],
            compiler_params=pltpu.CompilerParams(vmem_limit_bytes=16 * 1024 * 1024),
            name="hand_out",
        )(*made)

    in_specs = (P(("grp", "fs", "tp"), None), P("fs", "tp"), P("fs", "tp"), P("fs"))
    out_specs = (P("grp", "tp"), P(("grp", "tp"), None), P(("grp", "fs", "tp"), None))
    return jax.shard_map(on_device, mesh=mesh, in_specs=in_specs, out_specs=out_specs, check_vma=False)
```

```python
import functools

import jax
import jax.numpy as jnp
from jax import lax
from jax.experimental import pallas as pl
from jax.experimental.pallas import tpu as pltpu
from jax.sharding import PartitionSpec as P

MESH = pl.DeviceIdType.MESH
BF16 = jnp.bfloat16
F32 = jnp.float32
QUARTERS = 4
TOK_CHUNKS = 4
WEIGHT_CHUNKS = 2
WAYS = (1, -1)
REACH = (3, 5, 7, 8)
COPY_PARTS = 1
SEND_SEMS = ("own", "perm", "relay", "pass", "tok", "tokpair", "up", "uppair", "upacross", "dn", "dnpair", "dnacross", "rs")


def ring_messages(n, chunks):
    return (n // 2 - 1) * chunks + chunks // 2


def chunk_of(way, m, chunks):
    return (m + (0 if way == 1 else chunks // 2)) % chunks


def chain_start(j, way, half_x):
    return half_x if (j % 2 == 0) == (way == 1) else half_x - 1


def limit(way, c, half_z):
    return half_z if (c == 0) == (way == 1) else half_z - 1


def quarter_from(far):
    return sum(far > reach for reach in REACH[:-1])


def receive_numbers(n_z, n_x):
    half_z, half_x = n_z // 2, n_x // 2
    both = [("own",), ("uppair", 0)] + [("dnpair", quarter) for quarter in range(QUARTERS)]
    both += [
        ("rs", way, j, k) for way in WAYS for j in range(QUARTERS) for k in range(chain_start(j, way, half_x), 0, -1)
    ]
    core_0 = [("upacross", 0), ("upacross", 1)] + [("dnacross", quarter) for quarter in range(QUARTERS)]
    core_0 += [("tok", way, m) for way in WAYS for m in range(ring_messages(n_x, TOK_CHUNKS))]
    core_1 = [("perm",), ("relay",), ("tokpair",)]
    for kind in ("up", "dn"):
        core_1 += [
            (kind, way, far, c)
            for way in WAYS
            for c in range(WEIGHT_CHUNKS)
            for far in range(1, limit(way, c, half_z) + 1)
        ]
    number = {name: k for k, name in enumerate(both)}
    for names in (core_0, core_1):
        number |= {name: len(both) + k for k, name in enumerate(names)}
    return number


def kernel(
    number, slot, n_f, n_x,
    tok_in, up_in, dn_in, gain_in,
    up_all, dn_all, y_out,
    tok_v, up_v, dn_v, gain_v, stage, relay, tok_all, hid, part, rs_out, rs_in,
    send_sem, recv_sem, load_sem,
):
    x = lax.axis_index("tp")
    f = lax.axis_index("fs")
    z, core = f // 2, f % 2
    n_z, half_x = n_f // 2, n_x // 2
    rows, d = tok_in.shape
    up_rows, width = up_in.shape
    dn_rows, dn_cols = dn_in.shape
    q_cols = d // QUARTERS
    all_rows = n_x * rows

    group = lax.axis_index("grp")
    odd = group % 2

    def at(**where):
        return {"grp": group, "fs": f, "tp": x} | where

    x_peer = {way: at(tp=lax.rem(x + way + n_x, n_x)) for way in WAYS}
    z_peer = {hop: at(fs=lax.rem(f + 2 * hop + n_f, n_f)) for hop in (1, -1, 2, -2)}
    pair = at(fs=2 * z + 1 - core)
    z_hi, z_lo = z // 2, z % 2
    to_plane = lax.rem(x + half_x, n_x)
    relays = to_plane == n_x - 1
    perm_peer = at(tp=z_hi, fs=lax.rem(2 * to_plane + z_lo + 2 * (to_plane // (n_x - 1)), n_z) * 2 + 1)
    perm_source = at(tp=lax.rem(z_hi + half_x, n_x), fs=(2 * x + z_lo) * 2 + odd)
    relay_source = at(tp=lax.rem(n_x - 1 + half_x, n_x), fs=(2 * x + z_lo) * 2 + odd)
    first_planes, last_planes = z_hi == 0, z_hi == n_x - 1
    permutes = core == odd
    across = [at(grp=group + 1 - 2 * odd, fs=2 * z + c) for c in range(2)]

    def greet(peer):
        pl.semaphore_signal(barrier, inc=1, device_id=peer, device_id_type=MESH)

    barrier = pltpu.get_barrier_semaphore()
    for peer in (x_peer[1], x_peer[-1], pair):
        greet(peer)

    @pl.when(core == 0)
    def _():
        greet(across[1])

    @pl.when(core == 1)
    def _():
        for hop in z_peer:
            greet(z_peer[hop])

        @pl.when(jnp.logical_not(last_planes))
        def _():
            greet(perm_source)

        @pl.when(first_planes)
        def _():
            greet(relay_source)

    loads = [
        pltpu.make_async_copy(src, dst, load_sem.at[k])
        for k, (src, dst) in enumerate(((dn_in, dn_v), (tok_in, tok_v), (gain_in, gain_v), (up_in, up_v)))
    ]
    for load in loads:
        load.start()

    def up_at(zz, c):
        return up_all.at[pl.ds(pl.multiple_of((zz * 2 + c) * up_rows, up_rows), up_rows), :]

    def up_part(zz, c):
        size = up_rows // WEIGHT_CHUNKS
        return up_all.at[pl.ds(pl.multiple_of((zz * 2 + odd) * up_rows + c * size, size), size), :]

    def dn_at(zz, c):
        row = pl.multiple_of((lax.rem(zz, 2) * 2 + c) * dn_rows, dn_rows)
        col = pl.multiple_of(lax.rem(zz // 2 + half_x, n_x) * dn_cols, dn_cols)
        return dn_all.at[pl.ds(row, dn_rows), pl.ds(col, dn_cols)]

    def dn_part(zz, c):
        size = dn_rows // WEIGHT_CHUNKS
        row = pl.multiple_of((lax.rem(zz, 2) * 2 + odd) * dn_rows + c * size, size)
        col = pl.multiple_of(lax.rem(zz // 2 + half_x, n_x) * dn_cols, dn_cols)
        return dn_all.at[pl.ds(row, size), pl.ds(col, dn_cols)]

    def tok_at(xx, c):
        size = rows // 2
        row = pl.multiple_of((c % 2) * all_rows + xx * rows + (c // 2) * size, size)
        return tok_all.at[pl.ds(row, size), :]

    def tok_own(c):
        return tok_all.at[pl.ds(pl.multiple_of(c * all_rows + x * rows, rows), rows), :]

    def message(name, src, dst, peer, sem=None):
        return pltpu.make_async_remote_copy(
            src_ref=src,
            dst_ref=dst,
            send_sem=send_sem.at[SEND_SEMS.index(sem or name[0])],
            recv_sem=recv_sem.at[number[name]],
            device_id=peer,
            device_id_type=MESH,
        )

    def send(name, src, dst, peer, sem=None):
        message(name, src, dst, peer, sem).start()

    def wait_bytes(sem, ref):
        pltpu.make_async_copy(ref, ref, sem).wait()

    with jax.named_scope("own"):
        loads[1].wait()
        tokens = tok_v[...].astype(F32)
        scale = lax.rsqrt(jnp.mean(tokens * tokens, axis=-1, keepdims=True) + 1e-06)
        tok_own(core)[...] = (tokens * scale).astype(BF16)
        loads[0].wait()
        stage[...] = dn_v[...].astype(BF16)
        perm_dst = dn_all.at[
            pl.ds(pl.multiple_of((z_lo * 2 + core) * dn_rows, dn_rows), dn_rows),
            pl.ds(pl.multiple_of(x * dn_cols, dn_cols), dn_cols),
        ]
        loads[2].wait()
        loads[3].wait()
        square = (up_rows, up_rows)
        diagonal = lax.broadcasted_iota(jnp.int32, square, 0) == lax.broadcasted_iota(jnp.int32, square, 1)
        gain = jnp.sum(jnp.where(diagonal, jnp.broadcast_to(gain_v[...], square), 0.0), axis=1, keepdims=True)
        up_at(z, core)[...] = (gain * up_v[...]).astype(BF16)

    with jax.named_scope("barrier"):
        pl.semaphore_wait(barrier, 3 + 5 * core + jnp.where(permutes, 1, 0))

    def stream(kind, n, chunks, me, place, peers, onward):
        count = ring_messages(n, chunks)

        def block(way, m, away):
            owner = lax.rem(me - way * (m // chunks + away) + n, n)
            return place(owner, chunk_of(way, m, chunks))

        def forward(way, m):
            if m < count:
                ref = block(way, m, 0)
                send((kind, way, m), ref, ref, peers[way])

        def step(m):
            if 0 <= m < count:
                with jax.named_scope(f"{kind}{m}"):
                    for way in WAYS:
                        ref = block(way, m, 1)
                        message((kind, way, m), ref, ref, peers[way]).wait_recv()
                        forward(way, m + chunks)
                        for name, peer in onward(way, m):
                            send(name, ref, ref, peer)

        return count, forward, step

    tok_count, tok_forward, tok_step = stream(
        "tok", n_x, TOK_CHUNKS, x, tok_at, x_peer,
        lambda way, m: [(("tokpair",), pair)] if chunk_of(way, m, TOK_CHUNKS) % 2 else [],
    )

    half_z = n_z // 2
    weight_parts = [(way, c) for c in range(WEIGHT_CHUNKS) for way in WAYS]

    def weights(kind, part_at, block_at, whole, group_of, pair_group):
        def part(way, c, far):
            return part_at(lax.rem(z - way * far + n_z, n_z), c)

        def launch(way, c, far):
            ref = part(way, c, far)
            for hop in (2, 1):
                if far + hop <= limit(way, c, half_z):
                    send((kind, way, far + hop, c), ref, ref, z_peer[way * hop])

        def first():
            for way, c in weight_parts:
                launch(way, c, 0)

        def step(far):
            parts = [(way, c) for way, c in weight_parts if far <= limit(way, c, half_z)]
            with jax.named_scope(f"{kind}{far}"):
                for way, c in parts:
                    ref = part(way, c, far)
                    message((kind, way, far, c), ref, ref, z_peer[way]).wait_recv()
                    if far % 2 == 0:
                        launch(way, c, far)
                for way, c in parts:
                    ref = part(way, c, far)
                    send((kind + "across", group_of(far)), ref, ref, across[0])
                    send((kind + "pair", pair_group(far)), ref, ref, pair)

        def pass_on(group, start, stop, own=False):
            chips = [(way, far) for far in range(start, stop + 1) for way in (WAYS if far < half_z else (1,))]
            chips += [(1, 0)] if own else []
            with jax.named_scope(f"{kind}across{group}"):
                wait_bytes(
                    recv_sem.at[number[(kind + "across", group)]],
                    whole.at[pl.ds(0, len(chips) * up_rows * width // whole.shape[1]), :],
                )
                for way, far in chips:
                    ref = block_at(lax.rem(z - way * far + n_z, n_z), 1 - odd)
                    send((kind + "pair", pair_group(far)), ref, ref, pair)

        return first, step, pass_on

    up_first, up_step, up_pass_on = weights("up", up_part, up_at, up_all, lambda far: far > half_z // 2, lambda far: 0)
    dn_first, dn_step, dn_pass_on = weights("dn", dn_part, dn_at, dn_all, quarter_from, quarter_from)

    def permute():
        @pl.when(jnp.logical_and(permutes, jnp.logical_not(relays)))
        def _():
            send(("perm",), stage, perm_dst, perm_peer)

        @pl.when(jnp.logical_and(permutes, relays))
        def _():
            send(("relay",), stage, relay, perm_peer)

    @pl.when(core == 0)
    def _():
        permute()

        send(("own",), up_at(z, 0), up_at(z, 0), pair)
        tok_forward(1, 0)
        tok_forward(-1, 0)
        tok_forward(1, 2)
        tok_forward(-1, 2)
        with jax.named_scope("tokown"):
            message(("own",), tok_own(1), tok_own(1), pair).wait_recv()
        for m in (1, 3):
            tok_forward(1, m)
            tok_forward(-1, m)
        for m in range(tok_count):
            tok_step(m)
            if m == tok_count - 4:
                up_pass_on(0, 1, half_z // 2)
        up_pass_on(1, half_z // 2 + 1, half_z)
        with jax.named_scope("uppair"):
            wait_bytes(recv_sem.at[number[("uppair", 0)]], up_all.at[pl.ds(0, n_z * up_rows), :])

    @pl.when(core == 1)
    def _():
        permute()

        send(("own",), tok_own(1), tok_own(1), pair)

        @pl.when(odd == 1)
        def _():
            up_first()

        send(("uppair", 0), up_at(z, 1), up_at(z, 1), pair)
        with jax.named_scope("upown"):
            message(("own",), up_at(z, 0), up_at(z, 0), pair).wait_recv()

        @pl.when(odd == 0)
        def _():
            up_first()

        mine = dn_at(z, odd)

        def relayed():
            @pl.when(first_planes)
            def _():
                with jax.named_scope("relay"):
                    message(("relay",), relay, relay, perm_peer).wait_recv()
                send(("perm",), relay, dn_at(lax.rem(z - 2 + n_z, n_z), odd), z_peer[-2], "pass")

        def permuted():
            with jax.named_scope("perm"):
                message(("perm",), mine, mine, perm_peer).wait_recv()
            dn_first()
            send(("dnacross", 0), mine, mine, across[0])
            send(("dnpair", 0), mine, mine, pair)

        def permuted_early():
            @pl.when(jnp.logical_not(last_planes))
            def _():
                permuted()

        def permuted_late():
            @pl.when(last_planes)
            def _():
                permuted()

        for act, *far in (
            (up_step, 2, 1, 4, 3), (relayed,), (permuted_early,), (up_step, 6, 5), (permuted_late,),
            (up_step, 8, 7), (dn_step, 2, 1, 4, 3, 6, 5, 8, 7),
        ):
            if far:
                for distance in far:
                    act(distance)
            else:
                act()
        with jax.named_scope("tokpair"):
            wait_bytes(recv_sem.at[number[("tokpair",)]], tok_all.at[pl.ds(0, (n_x - 1) * rows), :])
        with jax.named_scope("uppair"):
            wait_bytes(recv_sem.at[number[("uppair", 0)]], up_all.at[pl.ds(0, (n_z - 1) * up_rows), :])

    pieces = 4
    piece = all_rows // pieces
    for p in range(pieces):
        with jax.named_scope(f"hid{p}"):
            own = pl.ds(pl.multiple_of(core * all_rows + p * piece, piece), piece)
            product = jnp.dot(tok_all[own, :], up_all[...], preferred_element_type=F32)
            rectified = jnp.maximum(product, 0.0)
            hid[pl.ds(p * piece, piece), :] = (rectified * rectified).astype(BF16)

    near = 2 * (lax.rem(z, QUARTERS) // 2) - 1
    own_quarter = z // QUARTERS + 2
    quarter = [lax.rem(own_quarter + QUARTERS + shift, QUARTERS) for shift in (0, near, -near, 2)]

    def columns(j):
        return pl.ds(pl.multiple_of(quarter[j] * q_cols, q_cols), q_cols)

    def rs_rows(xx):
        return pl.ds(pl.multiple_of(xx * rows, rows), rows)

    def send_rs(way, j, k):
        where = slot[(way, j, k)]
        total = part[j, rs_rows(lax.rem(x + way * k + n_x, n_x)), :]
        if k < chain_start(j, way, half_x):
            before = slot[(way, j, k + 1)]
            message(("rs", way, j, k + 1), rs_out.at[before], rs_in.at[before], x_peer[way]).wait_recv()
            total = total + rs_in[before].astype(F32)
        rs_out[where] = total.astype(BF16)
        send(("rs", way, j, k), rs_out.at[where], rs_in.at[where], x_peer[way])

    def begin(j):
        @pl.when(core == 0)
        def _():
            dn_pass_on(j, REACH[j - 1] + 1 if j else 1, REACH[j], own=j == 0)

        chips = 2 * (REACH[j] - (REACH[j - 1] if j else 0)) + (j == 0) - (j == QUARTERS - 1)
        with jax.named_scope(f"dnpair{j}"):
            wait_bytes(recv_sem.at[number[("dnpair", j)]], dn_all.at[pl.ds(0, chips * dn_rows * dn_cols // d), :])
        with jax.named_scope(f"part{j}"):
            part[j] = jnp.dot(hid[...], dn_all[:, columns(j)], preferred_element_type=F32)
        for way in WAYS:
            send_rs(way, j, chain_start(j, way, half_x))

    def go_on(j, later):
        with jax.named_scope(f"rs{j}r{later}"):
            for way in WAYS:
                k = chain_start(j, way, half_x) - later
                if k >= 1:
                    send_rs(way, j, k)

    def end(j):
        with jax.named_scope(f"end{j}"):
            total = part[j, rs_rows(x), :]
            for way in WAYS:
                here = slot[(way, j, 1)]
                message(("rs", way, j, 1), rs_out.at[here], rs_in.at[here], x_peer[way]).wait_recv()
                total = total + rs_in[here].astype(F32)
            y_out[:, columns(j)] = total.astype(BF16)

    begin(0)
    begin(1)
    begin(2)
    go_on(0, 1)
    begin(3)
    for j in range(1, QUARTERS):
        go_on(j, 1)
    for later in range(2, half_x):
        for j in range(QUARTERS):
            go_on(j, later)
    for j in range(QUARTERS):
        end(j)

    with jax.named_scope("drain"):

        def sent(kind, ref):
            wait_bytes(send_sem.at[SEND_SEMS.index(kind)], ref)

        def permute_sent():
            @pl.when(jnp.logical_and(permutes, jnp.logical_not(relays)))
            def _():
                sent("perm", stage)

            @pl.when(jnp.logical_and(permutes, relays))
            def _():
                sent("relay", stage)

        sent("rs", rs_out)
        sent("dnpair", dn_all.at[pl.ds(0, n_z * dn_rows * dn_cols // d), :])

        @pl.when(core == 0)
        def _():
            sent("own", up_at(z, 0))

            permute_sent()

            sent("tok", tok_all.at[pl.ds(0, 2 * tok_count * (rows // 2)), :])
            sent("tokpair", tok_all.at[pl.ds(0, (n_x - 1) * rows), :])
            sent("uppair", up_all.at[pl.ds(0, (n_z - 1) * up_rows), :])

        @pl.when(core == 1)
        def _():
            sent("own", tok_own(1))

            permute_sent()

            @pl.when(first_planes)
            def _():
                sent("pass", stage)

            for kind in ("up", "upacross"):
                sent(kind, up_all.at[pl.ds(0, (n_z - 1) * up_rows), :])
            sent("uppair", up_all.at[pl.ds(0, n_z * up_rows), :])
            sent("dn", dn_all.at[pl.ds(0, (n_z - 1) * dn_rows * dn_cols // d), :])
            sent("dnacross", dn_all.at[pl.ds(0, n_z * dn_rows * dn_cols // d), :])


def copier(*refs):
    count = len(refs) // 2
    sem = refs[-1]
    copies = []
    for src, dst in zip(refs[:count], refs[count:-1]):
        size = src.shape[0] // COPY_PARTS
        for k in range(COPY_PARTS):
            part = pl.ds(k * size, size)
            copies.append(pltpu.make_async_copy(src.at[part, :], dst.at[part, :], sem.at[len(copies)]))
    for copy in copies:
        copy.start()
    for copy in copies:
        copy.wait()


def solution(mesh):
    n_f, n_x = mesh.shape["fs"], mesh.shape["tp"]
    assert n_f == 4 * n_x and n_x == 8 and mesh.shape["grp"] % 2 == 0
    number = receive_numbers(n_f // 2, n_x)
    slots = [name[1:] for name in number if name[0] == "rs"]
    slot = {name: k for k, name in enumerate(slots)}

    def on_device(tokens, up_master, down_master, norm_gain):
        rows, d = tokens.shape
        up_rows, width = up_master.shape
        dn_rows, dn_cols = down_master.shape
        results = (
            jax.ShapeDtypeStruct((up_rows * n_f, width), BF16),
            jax.ShapeDtypeStruct((width, d), BF16),
            jax.ShapeDtypeStruct((rows, d), BF16),
        )
        in_hbm = pl.BlockSpec(memory_space=pltpu.HBM)
        in_vmem = pl.BlockSpec(memory_space=pltpu.VMEM)
        arrays = (tokens, up_master, down_master, norm_gain.reshape(1, up_rows))
        made = pl.pallas_call(
            functools.partial(kernel, number, slot, n_f, n_x),
            out_shape=results,
            in_specs=[in_hbm] * 4,
            out_specs=(in_vmem,) * 3,
            scratch_shapes=[
                pltpu.VMEM((rows, d), BF16),
                pltpu.VMEM((up_rows, width), F32),
                pltpu.VMEM((dn_rows, dn_cols), F32),
                pltpu.VMEM((1, up_rows), F32),
                pltpu.VMEM((dn_rows, dn_cols), BF16),
                pltpu.VMEM((dn_rows, dn_cols), BF16),
                pltpu.VMEM((2 * n_x * rows, d), BF16),
                pltpu.VMEM((n_x * rows, width), BF16),
                pltpu.VMEM((QUARTERS, n_x * rows, d // QUARTERS), F32),
                pltpu.VMEM((len(slots), rows, d // QUARTERS), BF16),
                pltpu.VMEM((len(slots), rows, d // QUARTERS), BF16),
                pltpu.SemaphoreType.DMA((len(SEND_SEMS),)),
                pltpu.SemaphoreType.DMA((max(number.values()) + 1,)),
                pltpu.SemaphoreType.DMA((4,)),
            ],
            compiler_params=pltpu.CompilerParams(
                collective_id=0, has_side_effects=True, vmem_limit_bytes=32 * 1024 * 1024
            ),
            name="handoff",
        )(*(pltpu.with_memory_space_constraint(a, pltpu.HBM) for a in arrays))
        return pl.pallas_call(
            copier,
            out_shape=results,
            in_specs=[in_vmem] * 3,
            out_specs=(in_hbm,) * 3,
            scratch_shapes=[pltpu.SemaphoreType.DMA((3 * COPY_PARTS,))],
            compiler_params=pltpu.CompilerParams(vmem_limit_bytes=16 * 1024 * 1024),
            name="hand_out",
        )(*made)

    in_specs = (P(("grp", "fs", "tp"), None), P("fs", "tp"), P("fs", "tp"), P("fs"))
    out_specs = (P("grp", "tp"), P(("grp", "tp"), None), P(("grp", "fs", "tp"), None))
    return jax.shard_map(on_device, mesh=mesh, in_specs=in_specs, out_specs=out_specs, check_vma=False)
```

```python
import functools

import jax
import jax.numpy as jnp
from jax import lax
from jax.experimental import pallas as pl
from jax.experimental.pallas import tpu as pltpu
from jax.sharding import PartitionSpec as P

MESH = pl.DeviceIdType.MESH
BF16 = jnp.bfloat16
F32 = jnp.float32
QUARTERS = 4
TOK_CHUNKS = 4
WEIGHT_CHUNKS = 2
WAYS = (1, -1)
REACH = (3, 5, 7, 8)
COPY_PARTS = 1
SEND_SEMS = ("own", "perm", "relay", "pass", "tok", "tokpair", "up", "uppair", "upacross", "dn", "dnpair", "dnacross", "rs")


def ring_messages(n, chunks):
    return (n // 2 - 1) * chunks + chunks // 2


def chunk_of(way, m, chunks):
    return (m + (0 if way == 1 else chunks // 2)) % chunks


def chain_start(j, way, half_x):
    return half_x if (j % 2 == 0) == (way == 1) else half_x - 1


def limit(way, c, half_z):
    return half_z if (c == 0) == (way == 1) else half_z - 1


def quarter_from(far):
    return sum(far > reach for reach in REACH[:-1])


def receive_numbers(n_z, n_x):
    half_z, half_x = n_z // 2, n_x // 2
    both = [("own",), ("uppair", 0)] + [("dnpair", quarter) for quarter in range(QUARTERS)]
    both += [
        ("rs", way, j, k) for way in WAYS for j in range(QUARTERS) for k in range(chain_start(j, way, half_x), 0, -1)
    ]
    core_0 = [("upacross", 0), ("upacross", 1)] + [("dnacross", quarter) for quarter in range(QUARTERS)]
    core_0 += [("tok", way, m) for way in WAYS for m in range(ring_messages(n_x, TOK_CHUNKS))]
    core_1 = [("perm",), ("relay",), ("tokpair",)]
    for kind in ("up", "dn"):
        core_1 += [
            (kind, way, far, c)
            for way in WAYS
            for c in range(WEIGHT_CHUNKS)
            for far in range(2, limit(way, c, half_z) + 1, 2)
        ]
        core_1 += [(kind, far) for far in range(1, half_z, 2)]
    number = {name: k for k, name in enumerate(both)}
    for names in (core_0, core_1):
        number |= {name: len(both) + k for k, name in enumerate(names)}
    return number


def kernel(
    number, slot, n_f, n_x,
    tok_in, up_in, dn_in, gain_in,
    up_all, dn_all, y_out,
    tok_v, up_v, dn_v, gain_v, stage, relay, tok_all, hid, part, rs_out, rs_in,
    send_sem, recv_sem, load_sem,
):
    x = lax.axis_index("tp")
    f = lax.axis_index("fs")
    z, core = f // 2, f % 2
    n_z, half_x = n_f // 2, n_x // 2
    rows, d = tok_in.shape
    up_rows, width = up_in.shape
    dn_rows, dn_cols = dn_in.shape
    q_cols = d // QUARTERS
    all_rows = n_x * rows

    group = lax.axis_index("grp")
    odd = group % 2

    def at(**where):
        return {"grp": group, "fs": f, "tp": x} | where

    x_peer = {way: at(tp=lax.rem(x + way + n_x, n_x)) for way in WAYS}
    z_peer = {hop: at(fs=lax.rem(f + 2 * hop + n_f, n_f)) for hop in (1, -1, 2, -2)}
    pair = at(fs=2 * z + 1 - core)
    z_hi, z_lo = z // 2, z % 2
    to_plane = lax.rem(x + half_x, n_x)
    relays = to_plane == n_x - 1
    perm_peer = at(tp=z_hi, fs=lax.rem(2 * to_plane + z_lo + 2 * (to_plane // (n_x - 1)), n_z) * 2 + 1)
    perm_source = at(tp=lax.rem(z_hi + half_x, n_x), fs=(2 * x + z_lo) * 2 + odd)
    relay_source = at(tp=lax.rem(n_x - 1 + half_x, n_x), fs=(2 * x + z_lo) * 2 + odd)
    first_planes, last_planes = z_hi == 0, z_hi == n_x - 1
    permutes = core == odd
    across = [at(grp=group + 1 - 2 * odd, fs=2 * z + c) for c in range(2)]

    def greet(peer):
        pl.semaphore_signal(barrier, inc=1, device_id=peer, device_id_type=MESH)

    barrier = pltpu.get_barrier_semaphore()
    for peer in (x_peer[1], x_peer[-1], pair):
        greet(peer)

    @pl.when(core == 0)
    def _():
        greet(across[1])

    @pl.when(core == 1)
    def _():
        for hop in z_peer:
            greet(z_peer[hop])

        @pl.when(jnp.logical_not(last_planes))
        def _():
            greet(perm_source)

        @pl.when(first_planes)
        def _():
            greet(relay_source)

    loads = [
        pltpu.make_async_copy(src, dst, load_sem.at[k])
        for k, (src, dst) in enumerate(((dn_in, dn_v), (tok_in, tok_v), (gain_in, gain_v), (up_in, up_v)))
    ]
    for load in loads:
        load.start()

    def up_at(zz, c):
        return up_all.at[pl.ds(pl.multiple_of((zz * 2 + c) * up_rows, up_rows), up_rows), :]

    def up_part(zz, c):
        size = up_rows // WEIGHT_CHUNKS
        return up_all.at[pl.ds(pl.multiple_of((zz * 2 + odd) * up_rows + c * size, size), size), :]

    def dn_at(zz, c):
        row = pl.multiple_of((lax.rem(zz, 2) * 2 + c) * dn_rows, dn_rows)
        col = pl.multiple_of(lax.rem(zz // 2 + half_x, n_x) * dn_cols, dn_cols)
        return dn_all.at[pl.ds(row, dn_rows), pl.ds(col, dn_cols)]

    def dn_part(zz, c):
        size = dn_rows // WEIGHT_CHUNKS
        row = pl.multiple_of((lax.rem(zz, 2) * 2 + odd) * dn_rows + c * size, size)
        col = pl.multiple_of(lax.rem(zz // 2 + half_x, n_x) * dn_cols, dn_cols)
        return dn_all.at[pl.ds(row, size), pl.ds(col, dn_cols)]

    def tok_at(xx, c):
        size = rows // 2
        row = pl.multiple_of((c % 2) * all_rows + xx * rows + (c // 2) * size, size)
        return tok_all.at[pl.ds(row, size), :]

    def tok_own(c):
        return tok_all.at[pl.ds(pl.multiple_of(c * all_rows + x * rows, rows), rows), :]

    def message(name, src, dst, peer, sem=None):
        return pltpu.make_async_remote_copy(
            src_ref=src,
            dst_ref=dst,
            send_sem=send_sem.at[SEND_SEMS.index(sem or name[0])],
            recv_sem=recv_sem.at[number[name]],
            device_id=peer,
            device_id_type=MESH,
        )

    def send(name, src, dst, peer, sem=None):
        message(name, src, dst, peer, sem).start()

    def wait_bytes(sem, ref):
        pltpu.make_async_copy(ref, ref, sem).wait()

    with jax.named_scope("own"):
        loads[1].wait()
        tokens = tok_v[...].astype(F32)
        scale = lax.rsqrt(jnp.mean(tokens * tokens, axis=-1, keepdims=True) + 1e-06)
        tok_own(core)[...] = (tokens * scale).astype(BF16)
        loads[0].wait()
        stage[...] = dn_v[...].astype(BF16)
        perm_dst = dn_all.at[
            pl.ds(pl.multiple_of((z_lo * 2 + core) * dn_rows, dn_rows), dn_rows),
            pl.ds(pl.multiple_of(x * dn_cols, dn_cols), dn_cols),
        ]
        loads[2].wait()
        loads[3].wait()
        square = (up_rows, up_rows)
        diagonal = lax.broadcasted_iota(jnp.int32, square, 0) == lax.broadcasted_iota(jnp.int32, square, 1)
        gain = jnp.sum(jnp.where(diagonal, jnp.broadcast_to(gain_v[...], square), 0.0), axis=1, keepdims=True)
        up_at(z, core)[...] = (gain * up_v[...]).astype(BF16)

    with jax.named_scope("barrier"):
        pl.semaphore_wait(barrier, 3 + 5 * core + jnp.where(permutes, 1, 0))

    def stream(kind, n, chunks, me, place, peers, onward):
        count = ring_messages(n, chunks)

        def block(way, m, away):
            owner = lax.rem(me - way * (m // chunks + away) + n, n)
            return place(owner, chunk_of(way, m, chunks))

        def forward(way, m):
            if m < count:
                ref = block(way, m, 0)
                send((kind, way, m), ref, ref, peers[way])

        def step(m):
            if 0 <= m < count:
                with jax.named_scope(f"{kind}{m}"):
                    for way in WAYS:
                        ref = block(way, m, 1)
                        message((kind, way, m), ref, ref, peers[way]).wait_recv()
                        forward(way, m + chunks)
                        for name, peer in onward(way, m):
                            send(name, ref, ref, peer)

        return count, forward, step

    tok_count, tok_forward, tok_step = stream(
        "tok", n_x, TOK_CHUNKS, x, tok_at, x_peer,
        lambda way, m: [(("tokpair",), pair)] if chunk_of(way, m, TOK_CHUNKS) % 2 else [],
    )

    half_z = n_z // 2
    weight_parts = [(way, c) for c in range(WEIGHT_CHUNKS) for way in WAYS]

    def weights(kind, part_at, block_at, whole, group_of, pair_group):
        def part(way, c, far):
            return part_at(lax.rem(z - way * far + n_z, n_z), c)

        def launch(way, c, far, hop):
            if far + hop <= limit(way, c, half_z):
                ref = part(way, c, far)
                name = (kind, way, far + 2, c) if hop == 2 else (kind, far + 1)
                send(name, ref, ref, z_peer[way * hop])

        def first():
            for hop in (2, 1):
                for way, c in weight_parts:
                    launch(way, c, 0, hop)

        def step(far):
            parts = [(way, c) for way, c in weight_parts if far <= limit(way, c, half_z)]
            with jax.named_scope(f"{kind}{far}"):
                if far % 2:
                    wait_bytes(
                        recv_sem.at[number[(kind, far)]],
                        whole.at[pl.ds(0, 2 * up_rows * width // whole.shape[1]), :],
                    )
                else:
                    for way, c in parts:
                        ref = part(way, c, far)
                        message((kind, way, far, c), ref, ref, z_peer[way]).wait_recv()
                        launch(way, c, far, 2)
                    for way, c in parts:
                        launch(way, c, far, 1)
                for way, c in parts:
                    ref = part(way, c, far)
                    send((kind + "across", group_of(far)), ref, ref, across[0])
                    send((kind + "pair", pair_group(far)), ref, ref, pair)

        def pass_on(group, start, stop, own=False):
            chips = [(way, far) for far in range(start, stop + 1) for way in (WAYS if far < half_z else (1,))]
            chips += [(1, 0)] if own else []
            with jax.named_scope(f"{kind}across{group}"):
                wait_bytes(
                    recv_sem.at[number[(kind + "across", group)]],
                    whole.at[pl.ds(0, len(chips) * up_rows * width // whole.shape[1]), :],
                )
                for way, far in chips:
                    ref = block_at(lax.rem(z - way * far + n_z, n_z), 1 - odd)
                    send((kind + "pair", pair_group(far)), ref, ref, pair)

        return first, step, pass_on

    up_first, up_step, up_pass_on = weights("up", up_part, up_at, up_all, lambda far: far > half_z // 2, lambda far: 0)
    dn_first, dn_step, dn_pass_on = weights("dn", dn_part, dn_at, dn_all, quarter_from, quarter_from)

    def permute():
        @pl.when(jnp.logical_and(permutes, jnp.logical_not(relays)))
        def _():
            send(("perm",), stage, perm_dst, perm_peer)

        @pl.when(jnp.logical_and(permutes, relays))
        def _():
            send(("relay",), stage, relay, perm_peer)

    pieces = n_x // 2
    piece = 2 * rows

    def hidden(k):
        with jax.named_scope(f"hid{k}"):
            start = lax.rem(x // 2 + k, pieces) * piece
            own = pl.ds(pl.multiple_of(core * all_rows + start, piece), piece)
            product = jnp.dot(tok_all[own, :], up_all[...], preferred_element_type=F32)
            rectified = jnp.maximum(product, 0.0)
            hid[pl.ds(pl.multiple_of(start, piece), piece), :] = (rectified * rectified).astype(BF16)

    @pl.when(core == 0)
    def _():
        permute()

        send(("own",), up_at(z, 0), up_at(z, 0), pair)
        tok_forward(1, 0)
        tok_forward(-1, 0)
        tok_forward(1, 2)
        tok_forward(-1, 2)
        with jax.named_scope("tokown"):
            message(("own",), tok_own(1), tok_own(1), pair).wait_recv()
        for m in (1, 3):
            tok_forward(1, m)
            tok_forward(-1, m)
        for m in range(tok_count):
            tok_step(m)
            if m == tok_count - 4:
                up_pass_on(0, 1, half_z // 2)
            if m == tok_count - 2:
                up_pass_on(1, half_z // 2 + 1, half_z)
                with jax.named_scope("uppair"):
                    wait_bytes(recv_sem.at[number[("uppair", 0)]], up_all.at[pl.ds(0, n_z * up_rows), :])
                for k in (0, 1, 3):
                    hidden(k)
        hidden(2)

    @pl.when(core == 1)
    def _():
        permute()

        send(("own",), tok_own(1), tok_own(1), pair)

        @pl.when(odd == 1)
        def _():
            up_first()

        send(("uppair", 0), up_at(z, 1), up_at(z, 1), pair)
        with jax.named_scope("upown"):
            message(("own",), up_at(z, 0), up_at(z, 0), pair).wait_recv()

        @pl.when(odd == 0)
        def _():
            up_first()

        mine = dn_at(z, odd)

        def relayed():
            @pl.when(first_planes)
            def _():
                with jax.named_scope("relay"):
                    message(("relay",), relay, relay, perm_peer).wait_recv()
                send(("perm",), relay, dn_at(lax.rem(z - 2 + n_z, n_z), odd), z_peer[-2], "pass")

        def permuted():
            with jax.named_scope("perm"):
                message(("perm",), mine, mine, perm_peer).wait_recv()
            dn_first()
            send(("dnacross", 0), mine, mine, across[0])
            send(("dnpair", 0), mine, mine, pair)

        def permuted_early():
            @pl.when(jnp.logical_not(last_planes))
            def _():
                permuted()

        def permuted_late():
            @pl.when(last_planes)
            def _():
                permuted()

        for act, *far in (
            (up_step, 2, 1, 4, 3), (relayed,), (permuted_early,), (up_step, 6, 5), (permuted_late,),
            (up_step, 8, 7), (dn_step, 2, 1, 4, 3, 6, 5),
        ):
            if far:
                for distance in far:
                    act(distance)
            else:
                act()
        with jax.named_scope("tokpair"):
            wait_bytes(recv_sem.at[number[("tokpair",)]], tok_all.at[pl.ds(0, (n_x - 1) * rows), :])
        with jax.named_scope("uppair"):
            wait_bytes(recv_sem.at[number[("uppair", 0)]], up_all.at[pl.ds(0, (n_z - 1) * up_rows), :])
        hidden(0)
        hidden(1)
        dn_step(8)
        dn_step(7)
        hidden(3)
        hidden(2)

    near = 2 * (lax.rem(z, QUARTERS) // 2) - 1
    own_quarter = z // QUARTERS + 2
    quarter = [lax.rem(own_quarter + QUARTERS + shift, QUARTERS) for shift in (0, near, -near, 2)]

    def columns(j):
        return pl.ds(pl.multiple_of(quarter[j] * q_cols, q_cols), q_cols)

    def rs_rows(xx):
        return pl.ds(pl.multiple_of(xx * rows, rows), rows)

    def send_rs(way, j, k):
        where = slot[(way, j, k)]
        total = part[j, rs_rows(lax.rem(x + way * k + n_x, n_x)), :]
        if k < chain_start(j, way, half_x):
            before = slot[(way, j, k + 1)]
            message(("rs", way, j, k + 1), rs_out.at[before], rs_in.at[before], x_peer[way]).wait_recv()
            total = total + rs_in[before].astype(F32)
        rs_out[where] = total.astype(BF16)
        send(("rs", way, j, k), rs_out.at[where], rs_in.at[where], x_peer[way])

    def begin(j):
        @pl.when(core == 0)
        def _():
            dn_pass_on(j, REACH[j - 1] + 1 if j else 1, REACH[j], own=j == 0)

        chips = 2 * (REACH[j] - (REACH[j - 1] if j else 0)) + (j == 0) - (j == QUARTERS - 1)
        with jax.named_scope(f"dnpair{j}"):
            wait_bytes(recv_sem.at[number[("dnpair", j)]], dn_all.at[pl.ds(0, chips * dn_rows * dn_cols // d), :])
        with jax.named_scope(f"part{j}"):
            part[j] = jnp.dot(hid[...], dn_all[:, columns(j)], preferred_element_type=F32)
        for way in WAYS:
            send_rs(way, j, chain_start(j, way, half_x))

    def go_on(j, later):
        with jax.named_scope(f"rs{j}r{later}"):
            for way in WAYS:
                k = chain_start(j, way, half_x) - later
                if k >= 1:
                    send_rs(way, j, k)

    def end(j):
        with jax.named_scope(f"end{j}"):
            total = part[j, rs_rows(x), :]
            for way in WAYS:
                here = slot[(way, j, 1)]
                message(("rs", way, j, 1), rs_out.at[here], rs_in.at[here], x_peer[way]).wait_recv()
                total = total + rs_in[here].astype(F32)
            y_out[:, columns(j)] = total.astype(BF16)

    begin(0)
    begin(1)
    begin(2)
    go_on(0, 1)
    begin(3)
    for j in range(1, QUARTERS):
        go_on(j, 1)
    for later in range(2, half_x):
        for j in range(QUARTERS):
            go_on(j, later)
    for j in range(QUARTERS):
        end(j)

    with jax.named_scope("drain"):

        def sent(kind, ref):
            wait_bytes(send_sem.at[SEND_SEMS.index(kind)], ref)

        def permute_sent():
            @pl.when(jnp.logical_and(permutes, jnp.logical_not(relays)))
            def _():
                sent("perm", stage)

            @pl.when(jnp.logical_and(permutes, relays))
            def _():
                sent("relay", stage)

        sent("rs", rs_out)
        sent("dnpair", dn_all.at[pl.ds(0, n_z * dn_rows * dn_cols // d), :])

        @pl.when(core == 0)
        def _():
            sent("own", up_at(z, 0))

            permute_sent()

            sent("tok", tok_all.at[pl.ds(0, 2 * tok_count * (rows // 2)), :])
            sent("tokpair", tok_all.at[pl.ds(0, (n_x - 1) * rows), :])
            sent("uppair", up_all.at[pl.ds(0, (n_z - 1) * up_rows), :])

        @pl.when(core == 1)
        def _():
            sent("own", tok_own(1))

            permute_sent()

            @pl.when(first_planes)
            def _():
                sent("pass", stage)

            for kind in ("up", "upacross"):
                sent(kind, up_all.at[pl.ds(0, (n_z - 1) * up_rows), :])
            sent("uppair", up_all.at[pl.ds(0, n_z * up_rows), :])
            sent("dn", dn_all.at[pl.ds(0, (n_z - 1) * dn_rows * dn_cols // d), :])
            sent("dnacross", dn_all.at[pl.ds(0, n_z * dn_rows * dn_cols // d), :])


def copier(*refs):
    count = len(refs) // 2
    sem = refs[-1]
    copies = []
    for src, dst in zip(refs[:count], refs[count:-1]):
        size = src.shape[0] // COPY_PARTS
        for k in range(COPY_PARTS):
            part = pl.ds(k * size, size)
            copies.append(pltpu.make_async_copy(src.at[part, :], dst.at[part, :], sem.at[len(copies)]))
    for copy in copies:
        copy.start()
    for copy in copies:
        copy.wait()


def solution(mesh):
    n_f, n_x = mesh.shape["fs"], mesh.shape["tp"]
    assert n_f == 4 * n_x and n_x == 8 and mesh.shape["grp"] % 2 == 0
    number = receive_numbers(n_f // 2, n_x)
    slots = [name[1:] for name in number if name[0] == "rs"]
    slot = {name: k for k, name in enumerate(slots)}

    def on_device(tokens, up_master, down_master, norm_gain):
        rows, d = tokens.shape
        up_rows, width = up_master.shape
        dn_rows, dn_cols = down_master.shape
        results = (
            jax.ShapeDtypeStruct((up_rows * n_f, width), BF16),
            jax.ShapeDtypeStruct((width, d), BF16),
            jax.ShapeDtypeStruct((rows, d), BF16),
        )
        in_hbm = pl.BlockSpec(memory_space=pltpu.HBM)
        in_vmem = pl.BlockSpec(memory_space=pltpu.VMEM)
        arrays = (tokens, up_master, down_master, norm_gain.reshape(1, up_rows))
        made = pl.pallas_call(
            functools.partial(kernel, number, slot, n_f, n_x),
            out_shape=results,
            in_specs=[in_hbm] * 4,
            out_specs=(in_vmem,) * 3,
            scratch_shapes=[
                pltpu.VMEM((rows, d), BF16),
                pltpu.VMEM((up_rows, width), F32),
                pltpu.VMEM((dn_rows, dn_cols), F32),
                pltpu.VMEM((1, up_rows), F32),
                pltpu.VMEM((dn_rows, dn_cols), BF16),
                pltpu.VMEM((dn_rows, dn_cols), BF16),
                pltpu.VMEM((2 * n_x * rows, d), BF16),
                pltpu.VMEM((n_x * rows, width), BF16),
                pltpu.VMEM((QUARTERS, n_x * rows, d // QUARTERS), F32),
                pltpu.VMEM((len(slots), rows, d // QUARTERS), BF16),
                pltpu.VMEM((len(slots), rows, d // QUARTERS), BF16),
                pltpu.SemaphoreType.DMA((len(SEND_SEMS),)),
                pltpu.SemaphoreType.DMA((max(number.values()) + 1,)),
                pltpu.SemaphoreType.DMA((4,)),
            ],
            compiler_params=pltpu.CompilerParams(
                collective_id=0, has_side_effects=True, vmem_limit_bytes=32 * 1024 * 1024
            ),
            name="handoff",
        )(*(pltpu.with_memory_space_constraint(a, pltpu.HBM) for a in arrays))
        return pl.pallas_call(
            copier,
            out_shape=results,
            in_specs=[in_vmem] * 3,
            out_specs=(in_hbm,) * 3,
            scratch_shapes=[pltpu.SemaphoreType.DMA((3 * COPY_PARTS,))],
            compiler_params=pltpu.CompilerParams(vmem_limit_bytes=16 * 1024 * 1024),
            name="hand_out",
        )(*made)

    in_specs = (P(("grp", "fs", "tp"), None), P("fs", "tp"), P("fs", "tp"), P("fs"))
    out_specs = (P("grp", "tp"), P(("grp", "tp"), None), P(("grp", "fs", "tp"), None))
    return jax.shard_map(on_device, mesh=mesh, in_specs=in_specs, out_specs=out_specs, check_vma=False)
```

```python
import functools

import jax
import jax.numpy as jnp
from jax import lax
from jax.experimental import pallas as pl
from jax.experimental.pallas import tpu as pltpu
from jax.sharding import PartitionSpec as P

MESH = pl.DeviceIdType.MESH
BF16 = jnp.bfloat16
F32 = jnp.float32
QUARTERS = 4
TOK_CHUNKS = 4
WEIGHT_CHUNKS = 2
WAYS = (1, -1)
REACH = (3, 5, 7, 8)
COPY_PARTS = 1
SEND_SEMS = ("own", "perm", "relay", "pass", "tok", "tokpair", "up", "uppair", "upacross", "dn", "dnpair", "dnacross", "rs")


def ring_messages(n, chunks):
    return (n // 2 - 1) * chunks + chunks // 2


def chunk_of(way, m, chunks):
    return (m + (0 if way == 1 else chunks // 2)) % chunks


def chain_start(j, way, half_x):
    return half_x if (j % 2 == 0) == (way == 1) else half_x - 1


def limit(way, c, half_z):
    return half_z if (c == 0) == (way == 1) else half_z - 1


def quarter_from(far):
    return sum(far > reach for reach in REACH[:-1])


def receive_numbers(n_z, n_x):
    half_z, half_x = n_z // 2, n_x // 2
    both = [("own",), ("uppair", 0)] + [("dnpair", quarter) for quarter in range(QUARTERS)]
    both += [
        ("rs", way, j, k) for way in WAYS for j in range(QUARTERS) for k in range(chain_start(j, way, half_x), 0, -1)
    ]
    core_0 = [("upacross", 0), ("upacross", 1)] + [("dnacross", quarter) for quarter in range(QUARTERS)]
    core_0 += [("tok", way, m) for way in WAYS for m in range(ring_messages(n_x, TOK_CHUNKS))]
    core_1 = [("perm",), ("relay",), ("tokpair",)]
    for kind in ("up", "dn"):
        core_1 += [
            (kind, way, far, c)
            for way in WAYS
            for c in range(WEIGHT_CHUNKS)
            for far in range(2, limit(way, c, half_z) + 1, 2)
        ]
        core_1 += [(kind, far) for far in range(1, half_z, 2)]
    number = {name: k for k, name in enumerate(both)}
    for names in (core_0, core_1):
        number |= {name: len(both) + k for k, name in enumerate(names)}
    return number


def kernel(
    number, slot, n_f, n_x,
    tok_in, up_in, dn_in, gain_in,
    up_all, dn_all, y_out,
    tok_v, up_v, dn_v, gain_v, stage, relay, tok_all, hid, part, rs_out, rs_in,
    send_sem, recv_sem, load_sem,
):
    x = lax.axis_index("tp")
    f = lax.axis_index("fs")
    z, core = f // 2, f % 2
    n_z, half_x = n_f // 2, n_x // 2
    rows, d = tok_in.shape
    up_rows, width = up_in.shape
    dn_rows, dn_cols = dn_in.shape
    q_cols = d // QUARTERS
    all_rows = n_x * rows

    group = lax.axis_index("grp")
    odd = group % 2

    def at(**where):
        return {"grp": group, "fs": f, "tp": x} | where

    x_peer = {way: at(tp=lax.rem(x + way + n_x, n_x)) for way in WAYS}
    z_peer = {hop: at(fs=lax.rem(f + 2 * hop + n_f, n_f)) for hop in (1, -1, 2, -2)}
    pair = at(fs=2 * z + 1 - core)
    z_hi, z_lo = z // 2, z % 2
    to_plane = lax.rem(x + half_x, n_x)
    relays = to_plane == n_x - 1
    perm_peer = at(tp=z_hi, fs=lax.rem(2 * to_plane + z_lo + 2 * (to_plane // (n_x - 1)), n_z) * 2 + 1)
    perm_source = at(tp=lax.rem(z_hi + half_x, n_x), fs=(2 * x + z_lo) * 2 + odd)
    relay_source = at(tp=lax.rem(n_x - 1 + half_x, n_x), fs=(2 * x + z_lo) * 2 + odd)
    first_planes, last_planes = z_hi == 0, z_hi == n_x - 1
    permutes = core == odd
    across = [at(grp=group + 1 - 2 * odd, fs=2 * z + c) for c in range(2)]

    def greet(peer):
        pl.semaphore_signal(barrier, inc=1, device_id=peer, device_id_type=MESH)

    barrier = pltpu.get_barrier_semaphore()
    for peer in (x_peer[1], x_peer[-1], pair):
        greet(peer)

    @pl.when(core == 0)
    def _():
        greet(across[1])

    @pl.when(core == 1)
    def _():
        for hop in z_peer:
            greet(z_peer[hop])

        @pl.when(jnp.logical_not(last_planes))
        def _():
            greet(perm_source)

        @pl.when(first_planes)
        def _():
            greet(relay_source)

    loads = [
        pltpu.make_async_copy(src, dst, load_sem.at[k])
        for k, (src, dst) in enumerate(((dn_in, dn_v), (tok_in, tok_v), (gain_in, gain_v), (up_in, up_v)))
    ]
    for load in loads:
        load.start()

    def up_at(zz, c):
        return up_all.at[pl.ds(pl.multiple_of((zz * 2 + c) * up_rows, up_rows), up_rows), :]

    def up_part(zz, c):
        size = up_rows // WEIGHT_CHUNKS
        return up_all.at[pl.ds(pl.multiple_of((zz * 2 + odd) * up_rows + c * size, size), size), :]

    def dn_at(zz, c):
        row = pl.multiple_of((lax.rem(zz, 2) * 2 + c) * dn_rows, dn_rows)
        col = pl.multiple_of(lax.rem(zz // 2 + half_x, n_x) * dn_cols, dn_cols)
        return dn_all.at[pl.ds(row, dn_rows), pl.ds(col, dn_cols)]

    def dn_part(zz, c):
        size = dn_rows // WEIGHT_CHUNKS
        row = pl.multiple_of((lax.rem(zz, 2) * 2 + odd) * dn_rows + c * size, size)
        col = pl.multiple_of(lax.rem(zz // 2 + half_x, n_x) * dn_cols, dn_cols)
        return dn_all.at[pl.ds(row, size), pl.ds(col, dn_cols)]

    def tok_at(xx, c):
        size = rows // 2
        row = pl.multiple_of((c % 2) * all_rows + xx * rows + (c // 2) * size, size)
        return tok_all.at[pl.ds(row, size), :]

    def tok_own(c):
        return tok_all.at[pl.ds(pl.multiple_of(c * all_rows + x * rows, rows), rows), :]

    def message(name, src, dst, peer, sem=None):
        return pltpu.make_async_remote_copy(
            src_ref=src,
            dst_ref=dst,
            send_sem=send_sem.at[SEND_SEMS.index(sem or name[0])],
            recv_sem=recv_sem.at[number[name]],
            device_id=peer,
            device_id_type=MESH,
        )

    def send(name, src, dst, peer, sem=None):
        message(name, src, dst, peer, sem).start()

    def wait_bytes(sem, ref):
        pltpu.make_async_copy(ref, ref, sem).wait()

    with jax.named_scope("own"):
        loads[1].wait()
        tokens = tok_v[...].astype(F32)
        scale = lax.rsqrt(jnp.mean(tokens * tokens, axis=-1, keepdims=True) + 1e-06)
        tok_own(core)[...] = (tokens * scale).astype(BF16)
        loads[0].wait()
        stage[...] = dn_v[...].astype(BF16)
        perm_dst = dn_all.at[
            pl.ds(pl.multiple_of((z_lo * 2 + core) * dn_rows, dn_rows), dn_rows),
            pl.ds(pl.multiple_of(x * dn_cols, dn_cols), dn_cols),
        ]
        loads[2].wait()
        loads[3].wait()
        square = (up_rows, up_rows)
        diagonal = lax.broadcasted_iota(jnp.int32, square, 0) == lax.broadcasted_iota(jnp.int32, square, 1)
        gain = jnp.sum(jnp.where(diagonal, jnp.broadcast_to(gain_v[...], square), 0.0), axis=1, keepdims=True)
        up_at(z, core)[...] = (gain * up_v[...]).astype(BF16)

    with jax.named_scope("barrier"):
        pl.semaphore_wait(barrier, 3 + 5 * core + jnp.where(permutes, 1, 0))

    def stream(kind, n, chunks, me, place, peers, onward):
        count = ring_messages(n, chunks)

        def block(way, m, away):
            owner = lax.rem(me - way * (m // chunks + away) + n, n)
            return place(owner, chunk_of(way, m, chunks))

        def forward(way, m):
            if m < count:
                ref = block(way, m, 0)
                send((kind, way, m), ref, ref, peers[way])

        def step(m):
            if 0 <= m < count:
                with jax.named_scope(f"{kind}{m}"):
                    for way in WAYS:
                        ref = block(way, m, 1)
                        message((kind, way, m), ref, ref, peers[way]).wait_recv()
                        forward(way, m + chunks)
                        for name, peer in onward(way, m):
                            send(name, ref, ref, peer)

        return count, forward, step

    tok_count, tok_forward, tok_step = stream(
        "tok", n_x, TOK_CHUNKS, x, tok_at, x_peer,
        lambda way, m: [(("tokpair",), pair)] if chunk_of(way, m, TOK_CHUNKS) % 2 else [],
    )

    half_z = n_z // 2
    weight_parts = [(way, c) for c in range(WEIGHT_CHUNKS) for way in WAYS]

    def weights(kind, part_at, block_at, whole, group_of, pair_group):
        def part(way, c, far):
            return part_at(lax.rem(z - way * far + n_z, n_z), c)

        def launch(way, c, far, hop):
            if far + hop <= limit(way, c, half_z):
                ref = part(way, c, far)
                name = (kind, way, far + 2, c) if hop == 2 else (kind, far + 1)
                send(name, ref, ref, z_peer[way * hop])

        def first():
            for hop in (2, 1):
                for way, c in weight_parts:
                    launch(way, c, 0, hop)

        def step(far):
            parts = [(way, c) for way, c in weight_parts if far <= limit(way, c, half_z)]
            with jax.named_scope(f"{kind}{far}"):
                if far % 2:
                    wait_bytes(
                        recv_sem.at[number[(kind, far)]],
                        whole.at[pl.ds(0, 2 * up_rows * width // whole.shape[1]), :],
                    )
                else:
                    for way, c in parts:
                        ref = part(way, c, far)
                        message((kind, way, far, c), ref, ref, z_peer[way]).wait_recv()
                        launch(way, c, far, 2)
                    for way, c in parts:
                        launch(way, c, far, 1)
                for way, c in parts:
                    ref = part(way, c, far)
                    send((kind + "across", group_of(far)), ref, ref, across[0])
                    send((kind + "pair", pair_group(far)), ref, ref, pair)

        def pass_on(group, start, stop, own=False):
            chips = [(way, far) for far in range(start, stop + 1) for way in (WAYS if far < half_z else (1,))]
            chips += [(1, 0)] if own else []
            with jax.named_scope(f"{kind}across{group}"):
                wait_bytes(
                    recv_sem.at[number[(kind + "across", group)]],
                    whole.at[pl.ds(0, len(chips) * up_rows * width // whole.shape[1]), :],
                )
                for way, far in chips:
                    ref = block_at(lax.rem(z - way * far + n_z, n_z), 1 - odd)
                    send((kind + "pair", pair_group(far)), ref, ref, pair)

        return first, step, pass_on

    up_first, up_step, up_pass_on = weights("up", up_part, up_at, up_all, lambda far: far > half_z // 2, lambda far: 0)
    dn_first, dn_step, dn_pass_on = weights("dn", dn_part, dn_at, dn_all, quarter_from, quarter_from)

    def permute():
        @pl.when(jnp.logical_and(permutes, jnp.logical_not(relays)))
        def _():
            send(("perm",), stage, perm_dst, perm_peer)

        @pl.when(jnp.logical_and(permutes, relays))
        def _():
            send(("relay",), stage, relay, perm_peer)

    pieces = n_x // 2
    piece = 2 * rows

    def hidden(k):
        with jax.named_scope(f"hid{k}"):
            start = lax.rem(x // 2 + k, pieces) * piece
            own = pl.ds(pl.multiple_of(core * all_rows + start, piece), piece)
            product = jnp.dot(tok_all[own, :], up_all[...], preferred_element_type=F32)
            rectified = jnp.maximum(product, 0.0)
            hid[pl.ds(pl.multiple_of(start, piece), piece), :] = (rectified * rectified).astype(BF16)

    @pl.when(core == 0)
    def _():
        permute()

        send(("own",), up_at(z, 0), up_at(z, 0), pair)
        tok_forward(1, 0)
        tok_forward(-1, 0)
        tok_forward(1, 2)
        tok_forward(-1, 2)
        with jax.named_scope("tokown"):
            message(("own",), tok_own(1), tok_own(1), pair).wait_recv()
        for m in (1, 3):
            tok_forward(1, m)
            tok_forward(-1, m)
        for m in range(tok_count):
            tok_step(m)
            if m == tok_count - 4:
                up_pass_on(0, 1, half_z // 2)
            if m == tok_count - 2:
                up_pass_on(1, half_z // 2 + 1, half_z)
                with jax.named_scope("uppair"):
                    wait_bytes(recv_sem.at[number[("uppair", 0)]], up_all.at[pl.ds(0, n_z * up_rows), :])
                for k in (0, 1, 3):
                    hidden(k)
        hidden(2)

    @pl.when(core == 1)
    def _():
        permute()

        send(("own",), tok_own(1), tok_own(1), pair)

        @pl.when(odd == 1)
        def _():
            up_first()

        send(("uppair", 0), up_at(z, 1), up_at(z, 1), pair)
        with jax.named_scope("upown"):
            message(("own",), up_at(z, 0), up_at(z, 0), pair).wait_recv()

        @pl.when(odd == 0)
        def _():
            up_first()

        mine = dn_at(z, odd)

        def relayed():
            @pl.when(first_planes)
            def _():
                with jax.named_scope("relay"):
                    message(("relay",), relay, relay, perm_peer).wait_recv()
                send(("perm",), relay, dn_at(lax.rem(z - 2 + n_z, n_z), odd), z_peer[-2], "pass")

        def permuted():
            with jax.named_scope("perm"):
                message(("perm",), mine, mine, perm_peer).wait_recv()
            dn_first()
            send(("dnacross", 0), mine, mine, across[0])
            send(("dnpair", 0), mine, mine, pair)

        def permuted_early():
            @pl.when(jnp.logical_not(last_planes))
            def _():
                permuted()

        def permuted_late():
            @pl.when(last_planes)
            def _():
                permuted()

        for act, *far in (
            (up_step, 2, 4, 1), (relayed,), (permuted_early,), (up_step, 6, 3), (permuted_late,),
            (up_step, 8, 5, 7), (dn_step, 2, 4, 1, 3, 6, 5),
        ):
            if far:
                for distance in far:
                    act(distance)
            else:
                act()
        with jax.named_scope("tokpair"):
            wait_bytes(recv_sem.at[number[("tokpair",)]], tok_all.at[pl.ds(0, (n_x - 1) * rows), :])
        with jax.named_scope("uppair"):
            wait_bytes(recv_sem.at[number[("uppair", 0)]], up_all.at[pl.ds(0, (n_z - 1) * up_rows), :])
        hidden(0)
        hidden(1)
        dn_step(8)
        dn_step(7)
        hidden(3)
        hidden(2)

    near = 2 * (lax.rem(z, QUARTERS) // 2) - 1
    own_quarter = z // QUARTERS + 2
    quarter = [lax.rem(own_quarter + QUARTERS + shift, QUARTERS) for shift in (0, near, -near, 2)]

    def columns(j):
        return pl.ds(pl.multiple_of(quarter[j] * q_cols, q_cols), q_cols)

    def rs_rows(xx):
        return pl.ds(pl.multiple_of(xx * rows, rows), rows)

    def send_rs(way, j, k):
        where = slot[(way, j, k)]
        total = part[j, rs_rows(lax.rem(x + way * k + n_x, n_x)), :]
        if k < chain_start(j, way, half_x):
            before = slot[(way, j, k + 1)]
            message(("rs", way, j, k + 1), rs_out.at[before], rs_in.at[before], x_peer[way]).wait_recv()
            total = total + rs_in[before].astype(F32)
        rs_out[where] = total.astype(BF16)
        send(("rs", way, j, k), rs_out.at[where], rs_in.at[where], x_peer[way])

    def begin(j):
        @pl.when(core == 0)
        def _():
            dn_pass_on(j, REACH[j - 1] + 1 if j else 1, REACH[j], own=j == 0)

        chips = 2 * (REACH[j] - (REACH[j - 1] if j else 0)) + (j == 0) - (j == QUARTERS - 1)
        with jax.named_scope(f"dnpair{j}"):
            wait_bytes(recv_sem.at[number[("dnpair", j)]], dn_all.at[pl.ds(0, chips * dn_rows * dn_cols // d), :])
        with jax.named_scope(f"part{j}"):
            part[j] = jnp.dot(hid[...], dn_all[:, columns(j)], preferred_element_type=F32)
        for way in WAYS:
            send_rs(way, j, chain_start(j, way, half_x))

    def go_on(j, later):
        with jax.named_scope(f"rs{j}r{later}"):
            for way in WAYS:
                k = chain_start(j, way, half_x) - later
                if k >= 1:
                    send_rs(way, j, k)

    def end(j):
        with jax.named_scope(f"end{j}"):
            total = part[j, rs_rows(x), :]
            for way in WAYS:
                here = slot[(way, j, 1)]
                message(("rs", way, j, 1), rs_out.at[here], rs_in.at[here], x_peer[way]).wait_recv()
                total = total + rs_in[here].astype(F32)
            y_out[:, columns(j)] = total.astype(BF16)

    begin(0)
    begin(1)
    begin(2)
    go_on(0, 1)
    begin(3)
    for j in range(1, QUARTERS):
        go_on(j, 1)
    for later in range(2, half_x):
        for j in range(QUARTERS):
            go_on(j, later)
    for j in range(QUARTERS):
        end(j)

    with jax.named_scope("drain"):

        def sent(kind, ref):
            wait_bytes(send_sem.at[SEND_SEMS.index(kind)], ref)

        def permute_sent():
            @pl.when(jnp.logical_and(permutes, jnp.logical_not(relays)))
            def _():
                sent("perm", stage)

            @pl.when(jnp.logical_and(permutes, relays))
            def _():
                sent("relay", stage)

        sent("rs", rs_out)
        sent("dnpair", dn_all.at[pl.ds(0, n_z * dn_rows * dn_cols // d), :])

        @pl.when(core == 0)
        def _():
            sent("own", up_at(z, 0))

            permute_sent()

            sent("tok", tok_all.at[pl.ds(0, 2 * tok_count * (rows // 2)), :])
            sent("tokpair", tok_all.at[pl.ds(0, (n_x - 1) * rows), :])
            sent("uppair", up_all.at[pl.ds(0, (n_z - 1) * up_rows), :])

        @pl.when(core == 1)
        def _():
            sent("own", tok_own(1))

            permute_sent()

            @pl.when(first_planes)
            def _():
                sent("pass", stage)

            for kind in ("up", "upacross"):
                sent(kind, up_all.at[pl.ds(0, (n_z - 1) * up_rows), :])
            sent("uppair", up_all.at[pl.ds(0, n_z * up_rows), :])
            sent("dn", dn_all.at[pl.ds(0, (n_z - 1) * dn_rows * dn_cols // d), :])
            sent("dnacross", dn_all.at[pl.ds(0, n_z * dn_rows * dn_cols // d), :])


def copier(*refs):
    count = len(refs) // 2
    sem = refs[-1]
    copies = []
    for src, dst in zip(refs[:count], refs[count:-1]):
        size = src.shape[0] // COPY_PARTS
        for k in range(COPY_PARTS):
            part = pl.ds(k * size, size)
            copies.append(pltpu.make_async_copy(src.at[part, :], dst.at[part, :], sem.at[len(copies)]))
    for copy in copies:
        copy.start()
    for copy in copies:
        copy.wait()


def solution(mesh):
    n_f, n_x = mesh.shape["fs"], mesh.shape["tp"]
    assert n_f == 4 * n_x and n_x == 8 and mesh.shape["grp"] % 2 == 0
    number = receive_numbers(n_f // 2, n_x)
    slots = [name[1:] for name in number if name[0] == "rs"]
    slot = {name: k for k, name in enumerate(slots)}

    def on_device(tokens, up_master, down_master, norm_gain):
        rows, d = tokens.shape
        up_rows, width = up_master.shape
        dn_rows, dn_cols = down_master.shape
        results = (
            jax.ShapeDtypeStruct((up_rows * n_f, width), BF16),
            jax.ShapeDtypeStruct((width, d), BF16),
            jax.ShapeDtypeStruct((rows, d), BF16),
        )
        in_hbm = pl.BlockSpec(memory_space=pltpu.HBM)
        in_vmem = pl.BlockSpec(memory_space=pltpu.VMEM)
        arrays = (tokens, up_master, down_master, norm_gain.reshape(1, up_rows))
        made = pl.pallas_call(
            functools.partial(kernel, number, slot, n_f, n_x),
            out_shape=results,
            in_specs=[in_hbm] * 4,
            out_specs=(in_vmem,) * 3,
            scratch_shapes=[
                pltpu.VMEM((rows, d), BF16),
                pltpu.VMEM((up_rows, width), F32),
                pltpu.VMEM((dn_rows, dn_cols), F32),
                pltpu.VMEM((1, up_rows), F32),
                pltpu.VMEM((dn_rows, dn_cols), BF16),
                pltpu.VMEM((dn_rows, dn_cols), BF16),
                pltpu.VMEM((2 * n_x * rows, d), BF16),
                pltpu.VMEM((n_x * rows, width), BF16),
                pltpu.VMEM((QUARTERS, n_x * rows, d // QUARTERS), F32),
                pltpu.VMEM((len(slots), rows, d // QUARTERS), BF16),
                pltpu.VMEM((len(slots), rows, d // QUARTERS), BF16),
                pltpu.SemaphoreType.DMA((len(SEND_SEMS),)),
                pltpu.SemaphoreType.DMA((max(number.values()) + 1,)),
                pltpu.SemaphoreType.DMA((4,)),
            ],
            compiler_params=pltpu.CompilerParams(
                collective_id=0, has_side_effects=True, vmem_limit_bytes=32 * 1024 * 1024
            ),
            name="handoff",
        )(*(pltpu.with_memory_space_constraint(a, pltpu.HBM) for a in arrays))
        return pl.pallas_call(
            copier,
            out_shape=results,
            in_specs=[in_vmem] * 3,
            out_specs=(in_hbm,) * 3,
            scratch_shapes=[pltpu.SemaphoreType.DMA((3 * COPY_PARTS,))],
            compiler_params=pltpu.CompilerParams(vmem_limit_bytes=16 * 1024 * 1024),
            name="hand_out",
        )(*made)

    in_specs = (P(("grp", "fs", "tp"), None), P("fs", "tp"), P("fs", "tp"), P("fs"))
    out_specs = (P("grp", "tp"), P(("grp", "tp"), None), P(("grp", "fs", "tp"), None))
    return jax.shard_map(on_device, mesh=mesh, in_specs=in_specs, out_specs=out_specs, check_vma=False)
```
